512 devices in a mesh: sp: 32 (over z, core), tp: 16 (over y, x).
Axes of the slice: x: 4, y: 4, z: 16, core: 2. Of those that a mesh axis runs over, the one named last changes fastest.
Arguments:
- receptance: bfloat16 [8192, 4096], P('sp', 'tp'), may hold values from -6 to 6
- key_vectors: bfloat16 [8192, 4096], P('sp', 'tp'), may hold values from -13 to 13
- value_vectors: bfloat16 [8192, 4096], P('sp', 'tp'), may hold values from -6 to 6
- decay_logits: bfloat16 [8192, 4096], P('sp', 'tp'), may hold values from -20 to 2
- rate_logits: bfloat16 [8192, 4096], P('sp', 'tp'), may hold values from -8 to 4
- gate_logits: bfloat16 [8192, 4096], P('sp', 'tp'), may hold values from -6 to 6
- group_gain: float32 [4096], P('tp'), may hold values from 0.1 to 1.9
- residual: bfloat16 [8192, 4096], P('sp', 'tp'), may hold values from -24 to 24
- mixer_out: bfloat16 [4096, 4096], P(None, 'tp'), may hold values from -0.09375 to 0.09375
- norm_gain: float32 [4096], P('tp'), may hold values from 0.1 to 1.9
- expert_ids: int32 [8192, 2], P('sp'), may hold values from 0 to 31, as said below
- route_weight: float32 [8192, 2], P('sp'), may hold values from 0.25 to 1
- expert_gate: bfloat16 [32, 4096, 1024], P('sp', 'tp'), may hold values from -0.09375 to 0.09375
- expert_up: bfloat16 [32, 4096, 1024], P('sp', 'tp'), may hold values from -0.09375 to 0.09375
- expert_down: bfloat16 [32, 1024, 4096], P('sp', None, 'tp'), may hold values from -0.1875 to 0.1875
Outputs:
- updated: bfloat16 [8192, 4096], P('sp', 'tp')
The draws below stay inside these ranges and needn't reach their ends.
Inputs may be any that keep to these rules, and one draw needn't show every extreme that they name: `expert_ids`: the experts of a row are different and lie in one group of 8 consecutive experts. In the rows of one index of sp (aligned blocks of 256 rows) no expert is named by more than 32 rows, and in every such block some expert is named by exactly 32 rows.
All inputs are finite; a program needn't handle non-finite values.
Results may differ from the reference program's by a relative error of at most 0.013.
Values may be sent and summed in bfloat16 or wider, within the bound.
A program may use at most 64 MiB of HBM per device.

```python
import math
import jax
import jax.numpy as jnp
from jax import lax

D = 4096
WIDTH = 4096
HEAD = 64
HEADS = 64
FF = 1024
GROUPS = 4
TOP = 2
TOK_SP = 256
EXPERTS = 32
GROUP_EXPERTS = 8
CAP = 32
SLOTS = 1024
TOKENS = 8192
CUTS = 16
DBLK = 256
N_SP = 32


def fast_heads(key, count):
    order = jax.random.permutation(jax.random.fold_in(key, 7101), HEADS)
    return order < count


def draw_decay_logits(key, part):
    flags = fast_heads(key, HEADS // 2)
    noise = 0.6 * jnp.clip(jax.random.normal(jax.random.fold_in(key, 2), (TOKENS, WIDTH), jnp.float32), -3.0, 3.0)
    per_head = jnp.where(flags, math.log(1.0 / 16.0), math.log(0.8 / TOKENS))
    base = jnp.repeat(per_head, HEAD)
    channel = 0.3 * jnp.clip(jax.random.normal(jax.random.fold_in(key, 3), (WIDTH,), jnp.float32), -3.0, 3.0)
    halves = TOKENS // (TOK_SP // 2)
    drift = jax.random.uniform(jax.random.fold_in(key, 4), (halves, 1), jnp.float32, -1.1, 1.1)
    drift = jnp.repeat(drift, TOK_SP // 2, axis=0)
    log_rate = jnp.minimum(base[None, :] + channel[None, :] + drift + noise, -0.7)
    shifted = log_rate + 0.5
    return (shifted - jnp.log1p(-jnp.exp(shifted))).astype(jnp.bfloat16)


def draw_rate_logits(key, part):
    flags = fast_heads(key, HEADS // 2)
    spread = 0.7 * jnp.clip(jax.random.normal(jax.random.fold_in(key, 5), (TOKENS, WIDTH), jnp.float32), -2.4, 2.4)
    mixed_channels = jax.random.bernoulli(jax.random.fold_in(key, 6), 0.5, (WIDTH,))
    strong = jnp.logical_or(jnp.repeat(flags, HEAD), mixed_channels)
    centre = jnp.where(strong, 2.3, -6.0)
    width_scale = jnp.where(strong, 1.0, 0.5)
    return (centre[None, :] + width_scale[None, :] * spread).astype(jnp.bfloat16)


def draw_key_vectors(key, part):
    direction = jnp.clip(jax.random.normal(jax.random.fold_in(key, 21), (HEADS, HEAD), jnp.float32), -3.0, 3.0)
    along = 1.0 + 0.4 * jnp.clip(jax.random.normal(jax.random.fold_in(key, 22), (TOKENS, HEADS), jnp.float32), -2.0, 2.0)
    rough = jnp.clip(jax.random.normal(jax.random.fold_in(key, 23), (TOKENS, HEADS, HEAD), jnp.float32), -4.0, 4.0)
    keys = 1.5 * along[:, :, None] * direction[None, :, :] + rough
    return keys.reshape(TOKENS, WIDTH).astype(jnp.bfloat16)


def draw_residual(key, part):
    column_blocks = max(D // 128, 1)
    scales = jnp.exp(jax.random.uniform(jax.random.fold_in(key, 11), (column_blocks,), jnp.float32, math.log(0.4), math.log(2.5)))
    scales = jnp.repeat(scales, D // column_blocks)
    base = jnp.clip(jax.random.normal(jax.random.fold_in(key, 12), (TOKENS, D), jnp.float32), -5.0, 5.0)
    return (base * scales[None, :]).astype(jnp.bfloat16)


def draw_expert_ids(key, part):
    anchor = jax.random.fold_in(key, 9001)
    full_group = jax.random.randint(jax.random.fold_in(anchor, 1), (), 0, GROUPS)
    full_lead = jax.random.randint(jax.random.fold_in(anchor, 2), (), 0, GROUP_EXPERTS)
    block_keys = jax.random.split(jax.random.fold_in(anchor, 3), TOKENS // TOK_SP)
    spots = jnp.arange(GROUPS, dtype=jnp.int32)
    others_width = max(GROUP_EXPERTS - 1, 1)

    def one_block(block_key):
        keys_here = jax.random.split(block_key, 5)
        order = jax.random.permutation(keys_here[0], TOK_SP).astype(jnp.int32)
        held = jax.random.randint(keys_here[1], (), CAP, TOK_SP // 2 + 1)
        shift = jax.random.randint(keys_here[2], (), 0, GROUPS - 1)
        leads = jax.random.randint(keys_here[3], (GROUPS,), 0, GROUP_EXPERTS)
        leads = jnp.where(spots == full_group, full_lead, leads)
        shuffles = jax.vmap(lambda subkey: jax.random.permutation(subkey, others_width))(jax.random.split(keys_here[4], GROUPS)).astype(jnp.int32)
        in_full = order < held
        others = order - held
        group = jnp.where(in_full, full_group, (full_group + 1 + (others + shift) % (GROUPS - 1)) % GROUPS)
        rank = jnp.where(in_full, order, others // (GROUPS - 1))
        lead = leads[group]
        shuffle_rows = shuffles[group]

        def other_expert(position):
            pick = jnp.take_along_axis(shuffle_rows, (position % others_width)[:, None], axis=1)[:, 0]
            return (lead + 1 + pick) % GROUP_EXPERTS
        early = rank < CAP
        late_pos = CAP + 2 * (rank - CAP)
        first_pick = jnp.where(early, lead, other_expert(late_pos))
        second_pick = jnp.where(early, other_expert(rank), other_expert(late_pos + 1))
        return jnp.stack([group * GROUP_EXPERTS + first_pick, group * GROUP_EXPERTS + second_pick], axis=1)
    chosen = jax.vmap(one_block)(block_keys)
    return chosen.reshape(TOKENS, TOP).astype(jnp.int32)


def block_levels(own_key, extent, pieces, least, top_value):
    def one(dim, parts):
        steps = jax.random.uniform(jax.random.fold_in(jax.random.fold_in(own_key, 6), dim), (parts,), jnp.float32, least / len(pieces), top_value / len(pieces))
        return jnp.repeat(jnp.exp(steps), extent[dim] // parts).reshape((-1,) + (1,) * (len(extent) - dim - 1))

    loudness = one(*pieces[0])
    for cut in pieces[1:]:
        loudness = loudness * one(*cut)
    return loudness


def normal_values(key, dims, width, bound, cuts=(), kind=jnp.bfloat16):
    values = jax.random.normal(key, dims, jnp.float32) * width
    if len(cuts) > 0:
        values = block_levels(key, dims, cuts, -0.22, 0.18) * values
    return jnp.clip(values, min=-bound, max=bound).astype(kind)


def setup_inputs(seed: int = 0) -> dict:
    key_list = jax.random.split(jax.random.key(seed), 16)
    return {
        "receptance": normal_values(key_list[0], (TOKENS, WIDTH), 1.0, 6.0, ((0, 32), (1, 16))),
        "key_vectors": draw_key_vectors(jax.random.fold_in(key_list[15], 71), 0),
        "value_vectors": normal_values(key_list[2], (TOKENS, WIDTH), 1.0, 6.0, ((0, 32), (1, 16))),
        "decay_logits": draw_decay_logits(jax.random.fold_in(key_list[15], 71), 0),
        "rate_logits": draw_rate_logits(jax.random.fold_in(key_list[15], 71), 0),
        "gate_logits": normal_values(key_list[5], (TOKENS, WIDTH), 1.5, 6.0, ((0, 32), (1, 16))),
        "group_gain": jnp.clip(1.0 + 0.18 * jax.random.normal(key_list[6], (WIDTH,), jnp.float32), 0.1, 1.9),
        "residual": draw_residual(jax.random.fold_in(key_list[15], 71), 0),
        "mixer_out": normal_values(key_list[8], (WIDTH, D), WIDTH ** -0.5, 0.09375, ((1, 16),)),
        "norm_gain": jnp.clip(1.0 + 0.18 * jax.random.normal(key_list[9], (D,), jnp.float32), 0.1, 1.9),
        "expert_ids": draw_expert_ids(jax.random.fold_in(key_list[15], 71), 0),
        "route_weight": jnp.clip(0.25 + 0.75 * jax.random.uniform(key_list[11], (TOKENS, TOP), jnp.float32) ** block_levels(key_list[11], (TOKENS, TOP), ((0, 32),), -0.2, 0.2), 0.25, 1.0),
        "expert_gate": normal_values(key_list[12], (EXPERTS, D, FF), D ** -0.5, 0.09375, ((0, 32), (1, 16))),
        "expert_up": normal_values(key_list[13], (EXPERTS, D, FF), D ** -0.5, 0.09375, ((0, 32), (1, 16))),
        "expert_down": normal_values(key_list[14], (EXPERTS, FF, D), FF ** -0.5, 0.1875, ((0, 32), (2, 16))),
    }


EPS_GROUP = 0.00064
EPS_NORM = 1e-06
HIGHEST = lax.Precision.HIGHEST

def by_heads(array):
    return array.astype(jnp.float32).reshape(array.shape[0], WIDTH // HEAD, HEAD)

def time_mix(receptance, key_vectors, value_vectors, decay_logits, rate_logits, gate_logits, group_gain):
    recept = by_heads(receptance)
    keyvec = by_heads(key_vectors)
    valvec = by_heads(value_vectors)
    decay = jnp.exp(-jnp.exp(-jax.nn.softplus(-by_heads(decay_logits)) - 0.5))
    unit_key = keyvec / jnp.sqrt(1.0 + lax.optimization_barrier(jnp.sum(keyvec * keyvec, axis=-1, keepdims=True)))
    correction = unit_key * jax.nn.sigmoid(by_heads(rate_logits))

    def advance(carried, inputs):
        recept_now, decay_now, key_now, value_now, unit_now, corr_now = inputs
        pulled = jnp.einsum('hij,hj->hi', carried, unit_now, precision=HIGHEST)
        carried = carried * decay_now[:, None, :] - pulled[:, :, None] * corr_now[:, None, :] + value_now[:, :, None] * key_now[:, None, :]
        return (carried, jnp.einsum('hij,hj->hi', carried, recept_now, precision=HIGHEST))
    initial = jnp.zeros((WIDTH // HEAD, HEAD, HEAD), jnp.float32)
    final_state, state_read = lax.scan(advance, initial, (recept, decay, keyvec, valvec, unit_key, correction))
    centred = state_read - lax.optimization_barrier(jnp.mean(state_read, axis=-1, keepdims=True))
    scaled = centred * lax.rsqrt(lax.optimization_barrier(jnp.mean(centred * centred, axis=-1, keepdims=True)) + EPS_GROUP)
    gated_out = scaled.reshape(TOKENS, WIDTH) * group_gain.astype(jnp.float32)[None, :] * jax.nn.sigmoid(gate_logits.astype(jnp.float32))
    return gated_out.astype(jnp.bfloat16)

def block_ranks(expert_ids):
    grouped = expert_ids.reshape(N_SP, TOK_SP * TOP)
    onehot = (grouped[:, :, None] == jnp.arange(EXPERTS, dtype=jnp.int32)[None, None, :]).astype(jnp.int32)
    earlier = jnp.cumsum(onehot, axis=1) - onehot
    return lax.optimization_barrier(jnp.sum(earlier * onehot, axis=2)).reshape(TOKENS, TOP).astype(jnp.int32)

def cut_product(chosen, matrix):
    rows_cut = chosen.astype(jnp.float32).reshape(chosen.shape[0], CUTS, DBLK)
    matrix_cut = matrix.astype(jnp.float32).reshape(CUTS, DBLK, matrix.shape[1])
    partials = jnp.einsum('scd,cdf->csf', rows_cut, matrix_cut)
    rounded = lax.optimization_barrier(partials.astype(jnp.bfloat16))
    return lax.optimization_barrier(jnp.sum(rounded.astype(jnp.float32), axis=0))

def reference(receptance, key_vectors, value_vectors, decay_logits, rate_logits, gate_logits, group_gain, residual, mixer_out, norm_gain, expert_ids, route_weight, expert_gate, expert_up, expert_down):
    mixed_rows = time_mix(receptance, key_vectors, value_vectors, decay_logits, rate_logits, gate_logits, group_gain)
    midway = (residual.astype(jnp.float32) + jnp.dot(mixed_rows, mixer_out, preferred_element_type=jnp.float32)).astype(jnp.bfloat16)
    midway_f = midway.astype(jnp.float32)
    inv_rms = lax.rsqrt(lax.optimization_barrier(jnp.mean(midway_f * midway_f, axis=1, keepdims=True)) + EPS_NORM)
    normed = (midway_f * norm_gain.astype(jnp.float32)[None, :] * inv_rms).astype(jnp.bfloat16)
    ranks = block_ranks(expert_ids)
    token_ids = jnp.arange(TOKENS, dtype=jnp.int32)
    within = ((token_ids // TOK_SP)[:, None] * CAP + ranks).astype(jnp.int32)
    owners = jnp.broadcast_to(token_ids[:, None], expert_ids.shape).astype(jnp.int32)
    slot_table = jnp.full((EXPERTS, SLOTS), TOKENS, jnp.int32).at[expert_ids, within].set(owners)
    slot_weight = jnp.zeros((EXPERTS, SLOTS), jnp.float32).at[expert_ids, within].set(route_weight.astype(jnp.float32))
    padded = jnp.concatenate([normed, jnp.zeros((1, D), jnp.bfloat16)], axis=0)

    def one_expert(running, inputs):
        table_row, weight_row, gate_mat, up_mat, down_mat = inputs
        chosen = padded[table_row]
        hidden = (jax.nn.silu(cut_product(chosen, gate_mat)) * cut_product(chosen, up_mat)).astype(jnp.bfloat16)
        result = jnp.dot(hidden, down_mat, preferred_element_type=jnp.float32).astype(jnp.bfloat16)
        running = running.at[table_row].add(result.astype(jnp.float32) * weight_row[:, None])
        return (running, None)
    routed, unused = lax.scan(one_expert, jnp.zeros((TOKENS + 1, D), jnp.float32), (slot_table, slot_weight, expert_gate, expert_up, expert_down))
    return (midway_f + routed[:TOKENS]).astype(jnp.bfloat16)
```

```python
import functools

import jax
import jax.numpy as jnp
from jax import lax
from jax.experimental import pallas as pl
from jax.experimental.pallas import tpu as pltpu
from jax.sharding import PartitionSpec as P

D = 4096
HEAD = 64
CHUNK = 128
EXP_HALF = 0.6065306597126334

NZ = 16
N_SP = 2 * NZ
SIDE = 4
N_TP = SIDE * SIDE
CAP = 32
PARTS = 4
POS = N_SP // PARTS
SUB = POS * CAP // N_TP

EPS_GROUP = 0.00064
EPS_NORM = 1e-06
MESH = pl.DeviceIdType.MESH

OFFSETS = [0]
for _near in range(1, NZ // 2):
    OFFSETS += [_near, -_near]
OFFSETS += [NZ // 2]
INVERSE = [OFFSETS.index(-o if o != NZ // 2 else o) for o in OFFSETS]


def split(x):
    hi = x.astype(jnp.bfloat16)
    lo = (x - hi.astype(jnp.float32)).astype(jnp.bfloat16)
    return hi, lo


def dot(a, b, dims):
    return lax.dot_general(a, b, (dims, ((), ())), preferred_element_type=jnp.float32)


NN = ((1,), (0,))
NT = ((1,), (1,))
TN = ((0,), (0,))


def dot3(a, b, dims=NN):
    return dot(a[0], b[0], dims) + (dot(a[0], b[1], dims) + dot(a[1], b[0], dims))


def dot2(a, b, dims=NN):
    return dot(a[0], b, dims) + dot(a[1], b, dims)


def sigmoid(x):
    return 1.0 / (1.0 + jnp.exp(-x))


def mix_kernel(r_ref, k_ref, v_ref, d_ref, a_ref, out_ref, state_ref):
    tokens = r_ref.shape[0]
    chunks = tokens // CHUNK
    row = lax.broadcasted_iota(jnp.int32, (CHUNK, CHUNK), 0)
    col = lax.broadcasted_iota(jnp.int32, (CHUNK, CHUNK), 1)
    strict = col < row
    causal = col <= row
    eye = jnp.where(col == row, 1.0, 0.0)
    ones_lower = jnp.where(causal, 1.0, 0.0).astype(jnp.bfloat16)
    low = lax.broadcasted_iota(jnp.int32, (CHUNK, 2 * HEAD), 1) < HEAD

    work = []
    for chunk in range(chunks):
        rows = pl.ds(chunk * CHUNK, CHUNK)
        recept = r_ref[rows, :].astype(jnp.float32)
        keyvec = k_ref[rows, :].astype(jnp.float32)
        logdec = -EXP_HALF * sigmoid(d_ref[rows, :].astype(jnp.float32))
        first, second = split(logdec)
        third = (logdec - first.astype(jnp.float32) - second.astype(jnp.float32)).astype(jnp.bfloat16)
        cum_in = dot(ones_lower, first, NN) + (
            dot(ones_lower, second, NN) + dot(ones_lower, third, NN)
        )
        cum_end = cum_in[CHUNK - 1 :, :]
        squares = keyvec * keyvec
        norms = jnp.where(
            low,
            jnp.sum(squares[:, :HEAD], axis=1, keepdims=True),
            jnp.sum(squares[:, HEAD:], axis=1, keepdims=True),
        )
        unit_key = keyvec * lax.rsqrt(1.0 + norms)
        correction = unit_key * sigmoid(a_ref[rows, :].astype(jnp.float32))
        growth = jnp.exp(-cum_in)
        tail = jnp.exp(cum_end - cum_in)
        r_scaled = recept * jnp.exp(cum_in)
        u_scaled = unit_key * jnp.exp(cum_in - logdec)
        queries = split(jnp.concatenate([u_scaled, r_scaled], axis=0))
        sources = split(jnp.concatenate([keyvec * growth, correction * growth], axis=0))
        tails = split(jnp.concatenate([keyvec * tail, -(correction * tail)], axis=0))
        keep = jnp.broadcast_to(jnp.exp(cum_end), (2 * HEAD, 2 * HEAD)).T
        values = v_ref[rows, :]
        for head in range(2):
            lanes = slice(head * HEAD, (head + 1) * HEAD)
            query = tuple(q[:, lanes] for q in queries)
            source = tuple(s[:, lanes] for s in sources)
            scores = dot3(query, source, NT)
            work.append(
                dict(
                    head=head,
                    chunk=chunk,
                    query=query,
                    tail=tuple(t[:, lanes] for t in tails),
                    keep=keep[lanes, :],
                    value=jnp.concatenate(
                        [values[:, lanes], jnp.zeros((CHUNK, HEAD), jnp.bfloat16)], axis=1
                    ),
                    key_both=split(
                        jnp.concatenate(
                            [
                                jnp.where(strict, scores[:CHUNK, :CHUNK], 0.0),
                                jnp.where(causal, scores[CHUNK:, :CHUNK], 0.0),
                            ],
                            axis=0,
                        )
                    ),
                    pull=jnp.where(strict, scores[:CHUNK, CHUNK:], 0.0),
                    corr_read=split(jnp.where(causal, scores[CHUNK:, CHUNK:], 0.0)),
                )
            )
    for item in work:
        item["inverse"] = eye - jnp.where(row // 2 == col // 2, item["pull"], 0.0)
        item["from_values"] = dot2(item["key_both"], item["value"])
    size = 2
    while size < CHUNK:
        joined = (row // (2 * size) == col // (2 * size)) & (row // size != col // size)
        halves = []
        for item in work:
            inverse = split(item["inverse"])
            between = split(jnp.where(joined, item["pull"], 0.0))
            halves.append((inverse, dot3(between, inverse)))
        for item, (inverse, half) in zip(work, halves):
            item["inverse"] = item["inverse"] - dot3(inverse, split(half))
        size *= 2
    key_row = lax.broadcasted_iota(jnp.int32, (HEAD, 2 * HEAD), 0)
    lane = lax.broadcasted_iota(jnp.int32, (HEAD, 2 * HEAD), 1)
    start = jnp.where(lane == key_row + HEAD, 1.0, 0.0)
    states = [start, start]
    for item in work:
        head = item["head"]
        state = states[head]
        from_start = dot3(item["query"], split(state)) + item["from_values"]
        pulled = dot3(split(item["inverse"]), split(from_start[:CHUNK]))
        pulled_parts = split(pulled)
        out_ref[pl.ds(item["chunk"] * CHUNK, CHUNK), pl.ds(head * 2 * HEAD, 2 * HEAD)] = (
            from_start[CHUNK:] - dot3(item["corr_read"], pulled_parts)
        )
        key_tail = tuple(t[:CHUNK] for t in item["tail"])
        corr_tail = tuple(t[CHUNK:] for t in item["tail"])
        states[head] = (
            item["keep"] * state
            + dot2(key_tail, item["value"], TN)
            + dot3(corr_tail, pulled_parts, TN)
        )
    for head in range(2):
        state_ref[pl.ds(head * HEAD, HEAD), :] = states[head].astype(jnp.bfloat16)


def mix(receptance, key_vectors, value_vectors, decay_logits, rate_logits):
    tokens_here, channels = receptance.shape
    pairs = channels // (2 * HEAD)
    wide = pl.BlockSpec((tokens_here, 2 * HEAD), lambda i: (0, i))
    double = pl.BlockSpec((tokens_here, 4 * HEAD), lambda i: (0, i))
    return pl.pallas_call(
        mix_kernel,
        grid=(pairs,),
        in_specs=[wide] * 5,
        out_specs=[double, pl.BlockSpec((2 * HEAD, 2 * HEAD), lambda i: (i, 0))],
        out_shape=[
            jax.ShapeDtypeStruct((tokens_here, 2 * channels), jnp.float32),
            jax.ShapeDtypeStruct((channels, 2 * HEAD), jnp.bfloat16),
        ],
        name="mix",
    )(receptance, key_vectors, value_vectors, decay_logits, rate_logits)


def route_kernel(place_ref, ids_ref, weight_ref, pick_ref, high_ref, low_ref):
    tokens = ids_ref.shape[0]
    slots = N_SP * CAP
    expert = lax.broadcasted_iota(jnp.int32, (tokens, 128), 1)
    named = [ids_ref[:, k : k + 1] == expert for k in range(2)]
    onehot = jnp.where(named[0] | named[1], 1.0, 0.0).astype(jnp.bfloat16)
    row = lax.broadcasted_iota(jnp.int32, (tokens, tokens), 0)
    col = lax.broadcasted_iota(jnp.int32, (tokens, tokens), 1)
    before = jnp.where(col < row, 1.0, 0.0).astype(jnp.bfloat16)
    earlier = dot(before, onehot, NN).astype(jnp.bfloat16)
    weight = jnp.where(named[0], weight_ref[:, 0:1], 0.0) + jnp.where(named[1], weight_ref[:, 1:2], 0.0)
    high, low = split(weight)
    slot = lax.broadcasted_iota(jnp.int32, (128, slots), 1)
    source = lax.broadcasted_iota(jnp.int32, (128, slots), 0)
    near = slot // (2 * CAP)
    step = (near + 1) // 2
    off = jnp.where(near % 2 == 1, step, NZ - step)
    chip = (place_ref[0] // 2 + off) % NZ
    core = (place_ref[0] + slot // CAP) % 2
    spread = jnp.where(source == chip * 2 + core, 1.0, 0.0).astype(jnp.bfloat16)
    rank = (lax.broadcasted_iota(jnp.int32, (tokens, slots), 1) % CAP).astype(jnp.float32)
    taken = jnp.where(dot(earlier, spread, NN) == rank, dot(onehot, spread, NN), 0.0)
    pick_ref[...] = taken.T.astype(jnp.bfloat16)
    high_ref[...] = (taken * dot(high, spread, NN)).astype(jnp.bfloat16)
    low_ref[...] = (taken * dot(low, spread, NN)).astype(jnp.bfloat16)


def route(expert_ids, route_weight):
    tokens = expert_ids.shape[0]
    slots = N_SP * CAP
    place = lax.axis_index("sp").astype(jnp.int32).reshape(1)
    return pl.pallas_call(
        route_kernel,
        in_specs=[
            pl.BlockSpec(memory_space=pltpu.SMEM),
            pl.BlockSpec(memory_space=pltpu.VMEM),
            pl.BlockSpec(memory_space=pltpu.VMEM),
        ],
        out_shape=[
            jax.ShapeDtypeStruct((slots, tokens), jnp.bfloat16),
            jax.ShapeDtypeStruct((tokens, slots), jnp.bfloat16),
            jax.ShapeDtypeStruct((tokens, slots), jnp.bfloat16),
        ],
        name="route",
    )(place, expert_ids, route_weight)


class Place:
    def __init__(self):
        self.sp = lax.axis_index("sp")
        self.tp = lax.axis_index("tp")
        self.z, self.core = self.sp // 2, self.sp % 2
        self.y, self.x = self.tp // SIDE, self.tp % SIDE

    def chip(self, off, other=False):
        core = (self.core + 1) % 2 if other else self.core
        return ((self.z + off + NZ) % NZ) * 2 + core

    def at_z(self, off, other=False):
        return {"sp": self.chip(off, other), "tp": self.tp}

    def along(self, axis, off):
        if axis == "x":
            return {"sp": self.sp, "tp": self.y * SIDE + (self.x + off + SIDE) % SIDE}
        return {"sp": self.sp, "tp": ((self.y + off + SIDE) % SIDE) * SIDE + self.x}

    def on(self, axis, off=0):
        return ((self.x if axis == "x" else self.y) + off + SIDE) % SIDE


class Copies:
    def __init__(self, send, recv):
        self.send, self.recv = send, recv
        self.made = []

    def __call__(self, src, dst, device):
        index = len(self.made)
        copy = pltpu.make_async_remote_copy(
            src_ref=src,
            dst_ref=dst,
            send_sem=self.send.at[index],
            recv_sem=self.recv.at[index],
            device_id=device,
            device_id_type=MESH,
        )
        self.made.append(copy)
        return copy

    def drain(self):
        for copy in self.made:
            copy.wait_send()


def greet(devices):
    barrier = pltpu.get_barrier_semaphore()
    for device in devices:
        pl.semaphore_signal(barrier, inc=1, device_id=device, device_id_type=MESH)
    return lambda: pl.semaphore_wait(barrier, len(devices))


ORDER = (("x", "y"), ("y", "x"))


class TorusGather:
    def __init__(self, place, copies, blocks):
        self.place, self.copies, self.blocks = place, copies, blocks
        self.state = [dict() for _ in blocks]

    def own(self, h):
        first, second = ORDER[h]
        return self.place.on(second) * SIDE + self.place.on(first)

    def exchange(self, h, axis, mine):
        up, down = self.place.along(axis, 1), self.place.along(axis, -1)
        whole = mine(0)
        direct = [self.copies(whole, whole, up), self.copies(whole, whole, down)]
        for copy in direct:
            copy.start()
        return direct, up, down

    def relay(self, direct, up, down, mine, half):
        passed = []
        for side, (copy, off, target) in enumerate(zip(direct, (-1, 1), (up, down))):
            copy.wait_recv()
            piece = half(mine(off), side)
            passed.append(self.copies(piece, piece, target))
            passed[-1].start()
        return passed

    def stage(self, n, h):
        first, second = ORDER[h]
        place, block, s = self.place, self.blocks[h], self.state[h]

        def one(off):
            return block.at[place.on(second) * SIDE + place.on(first, off)]

        def four(off):
            return block.at[pl.ds(place.on(second, off) * SIDE, SIDE)]

        if n == 0:
            s["a"] = self.exchange(h, first, one)
        elif n == 1:
            s["b"] = self.relay(*s["a"], one, lambda ref, side: ref.at[side])
        elif n == 2:
            for copy in s["b"]:
                copy.wait_recv()
            s["c"] = self.exchange(h, second, four)
        elif n == 3:
            s["d"] = self.relay(*s["c"], four, lambda ref, side: ref.at[:, side])
        else:
            for copy in s["d"]:
                copy.wait_recv()


def torus_order(h):
    if h == 0:
        return list(range(N_TP))
    return [x * SIDE + y for y in range(SIDE) for x in range(SIDE)]


def front_kernel(
    reads_ref, states_ref, gate_ref, gain_ref, weight_ref, residual_ref,
    out_ref, maps, half_a, half_b, send, recv,
):
    place = Place()
    copies = Copies(send, recv)
    partner = place.at_z(0, True)
    up, down = place.at_z(1), place.at_z(-1)
    neighbours = [partner, up, down] + [place.along(axis, off) for axis in "xy" for off in (1, -1)]
    wait = greet(neighbours)
    tokens = out_ref.shape[0]
    pieces = 2
    rows = states_ref.shape[0] // pieces
    maps[place.sp] = states_ref[...]
    wait()

    def slot(off):
        return place.chip(off)

    def hop(n, direction, piece):
        part = pl.ds(piece * rows, rows)
        target = up if direction > 0 else down
        here = slot(-direction * (n - 1))
        src = states_ref.at[part] if n == 1 else maps.at[here, part]
        copy = copies(src, maps.at[here, part], target)
        copy.start()
        return copy

    across = [copies(states_ref, maps.at[slot(0)], partner)]
    last = {1: NZ // 2, -1: NZ // 2 - 1}
    current = {}
    for piece in range(pieces):
        for direction in (1, -1):
            current[direction, piece] = hop(1, direction, piece)
    across[0].start()
    for n in range(1, NZ // 2 + 1):
        for piece in range(pieces):
            for direction in (1, -1):
                if n > last[direction]:
                    continue
                current[direction, piece].wait_recv()
                if n < last[direction]:
                    current[direction, piece] = hop(n + 1, direction, piece)
        for direction in (1, -1):
            if n <= last[direction]:
                here = slot(-direction * n)
                copy = copies(maps.at[here], maps.at[here], partner)
                copy.start()
                across.append(copy)
    for copy in across:
        copy.wait_recv()

    heads = states_ref.shape[0] // HEAD

    def fold(step, carried):
        following = []
        for head in range(heads):
            both = maps[step, pl.ds(head * HEAD, HEAD), :]
            hi, lo = split(carried[head])
            step_map = both[:, HEAD:]
            following.append(
                both[:, :HEAD].astype(jnp.float32) + dot(step_map, hi, NN) + dot(step_map, lo, NN)
            )
        return tuple(following)

    zero = jnp.zeros((HEAD, HEAD), jnp.float32)
    incoming = lax.fori_loop(0, place.sp, fold, (zero,) * heads)
    scaled = []
    for head in range(heads):
        both = reads_ref[:, pl.ds(head * 2 * HEAD, 2 * HEAD)]
        state_read = both[:, :HEAD] + dot3(split(both[:, HEAD:]), split(incoming[head]))
        centred = state_read - jnp.mean(state_read, axis=1, keepdims=True)
        variance = jnp.mean(centred * centred, axis=1, keepdims=True)
        scaled.append(centred * lax.rsqrt(variance + EPS_GROUP))
    gated = (
        jnp.concatenate(scaled, axis=1)
        * gain_ref[...]
        * sigmoid(gate_ref[...].astype(jnp.float32))
    ).astype(jnp.bfloat16)
    halves = (half_a, half_b)
    gather = TorusGather(place, copies, halves)
    quarter = tokens // 4
    for h in range(2):
        for q in range(2):
            at = (2 * h + q) * quarter
            halves[h][gather.own(h), q] = gated[at : at + quarter]
    for n in range(5):
        for h in range(2):
            gather.stage(n, h)
    width = gated.shape[1]
    for h in range(2):
        total = jnp.zeros((tokens // 2, out_ref.shape[1]), jnp.float32)
        for t, at in enumerate(torus_order(h)):
            block = halves[h][at].reshape(tokens // 2, width)
            total += dot(block, weight_ref[pl.ds(t * width, width), :], NN)
        part = pl.ds(h * (tokens // 2), tokens // 2)
        out_ref[part, :] = (residual_ref[part, :].astype(jnp.float32) + total).astype(jnp.bfloat16)
    copies.drain()


def front(reads, states, gate_logits, group_gain, mixer_out, residual):
    tokens, channels = gate_logits.shape
    quarter = tokens // 4
    count = 64
    vmem = pl.BlockSpec(memory_space=pltpu.VMEM)
    return pl.pallas_call(
        front_kernel,
        in_specs=[vmem] * 6,
        out_specs=vmem,
        out_shape=jax.ShapeDtypeStruct(residual.shape, jnp.bfloat16),
        scratch_shapes=[
            pltpu.VMEM((N_SP, *states.shape), jnp.bfloat16),
            pltpu.VMEM((N_TP, 2, quarter, channels), jnp.bfloat16),
            pltpu.VMEM((N_TP, 2, quarter, channels), jnp.bfloat16),
            pltpu.SemaphoreType.DMA((count,)),
            pltpu.SemaphoreType.DMA((count,)),
        ],
        compiler_params=pltpu.CompilerParams(collective_id=0, has_side_effects=True),
        name="front",
    )(reads, states, gate_logits, group_gain.reshape(1, channels), mixer_out, residual)


EXTRA = 128


def widths(ff):
    return ((ff // 2 + EXTRA, ff // 2), (ff // 2, ff // 2))


def back_scratch(ff, features):
    wide = widths(ff)
    per_part = []
    for h in range(2):
        for q in range(2):
            w = wide[h][q]
            per_part += [
                pltpu.VMEM((PARTS, N_TP, SUB, w), jnp.bfloat16),
                pltpu.VMEM((PARTS, SIDE, SUB, w), jnp.bfloat16),
                pltpu.VMEM((PARTS, 2, SIDE, SUB, w), jnp.bfloat16),
                pltpu.VMEM((PARTS, SIDE, SUB, w), jnp.bfloat16),
                pltpu.VMEM((PARTS, SUB, w), jnp.bfloat16),
                pltpu.VMEM((PARTS, 2, SUB, w), jnp.bfloat16),
            ]
    hidden = [pltpu.VMEM((PARTS, N_TP, 2, SUB, ff // 4), jnp.bfloat16) for _ in range(2)]
    slots = [pltpu.VMEM((N_SP, CAP, features), jnp.bfloat16) for _ in range(4)]
    count = 2 * (N_SP - 1) + PARTS * (24 + 16)
    return slots + hidden + per_part + [
        pltpu.SemaphoreType.DMA((count,)),
        pltpu.SemaphoreType.DMA((count,)),
    ]


REDUCE = (("y", "x"), ("x", "y"))


def back_kernel(
    mid_ref, gain_ref, pick_ref, high_ref, low_ref, gate_ref, up_ref, down_ref, out_ref, *scratch
):
    outgoing, arrived, results, returned = scratch[:4]
    hidden = scratch[4:6]
    buffers = [[scratch[6 + (2 * h + q) * 6 : 12 + (2 * h + q) * 6] for q in range(2)] for h in range(2)]
    send, recv = scratch[30:]
    place = Place()
    copies = Copies(send, recv)
    features = mid_ref.shape[1]
    ff = gate_ref.shape[1]
    half = ff // 2
    z_peers = [
        (2 * near + other, 2 * INVERSE[near] + other, place.at_z(off, bool(other)))
        for near, off in enumerate(OFFSETS)
        for other in range(2)
        if off != 0 or other
    ]
    ring = [place.along(axis, off) for axis in "xy" for off in (1, -1)]
    wait = greet([peer[2] for peer in z_peers] + ring)
    for part in range(PARTS):
        rows = pl.ds(part * POS * CAP, POS * CAP)
        outgoing[pl.ds(part * POS, POS)] = (
            dot(pick_ref[rows, :], mid_ref[...], NN).astype(jnp.bfloat16).reshape(POS, CAP, features)
        )
    arrived[0] = outgoing[0]
    wait()
    dispatch = {}
    for at, there, device in z_peers:
        dispatch[at] = copies(outgoing.at[at], arrived.at[there], device)
        dispatch[at].start()
    lands = {there: dispatch[at] for at, there, _ in z_peers}
    back = {}
    state = [dict() for _ in range(PARTS)]
    gathers = [
        TorusGather(place, copies, [hidden[h].at[part] for h in range(2)]) for part in range(PARTS)
    ]

    def add(*refs):
        total = refs[0].astype(jnp.float32)
        for ref in refs[1:]:
            total += ref.astype(jnp.float32)
        return total

    def relay_out(part, h, level):
        axis = REDUCE[h][level]
        far = place.on(axis, 2)
        sent = []
        for q, off in ((0, 1), (1, -1)):
            product, passed1, _, reduced, passed2, _ = buffers[h][q]
            if level == 0:
                src, dst = product.at[part, pl.ds(far * SIDE, SIDE)], passed1.at[part]
            else:
                src, dst = reduced.at[part, far], passed2.at[part]
            copy = copies(src, dst, place.along(axis, off))
            copy.start()
            sent.append(copy)
        state[part][h, level, "relay"] = sent

    def join(part, h, level):
        axis = REDUCE[h][level]
        sent = []
        for side, off in ((0, 1), (1, -1)):
            state[part][h, level, "relay"][side].wait_recv()
            near = place.on(axis, off)
            for q in (side, 1 - side):
                product, passed1, both1, reduced, passed2, both2 = buffers[h][q]
                if level == 0:
                    at, mine, dst = pl.ds(near * SIDE, SIDE), product, both1.at[part, side]
                    other = passed1
                else:
                    at, mine, dst = near, reduced, both2.at[part, side]
                    other = passed2
                if q == side:
                    mine[part, at] = add(mine[part, at], other[part]).astype(jnp.bfloat16)
                copy = copies(mine.at[part, at], dst, place.along(axis, off))
                copy.start()
                sent.append(copy)
        state[part][h, level, "both"] = sent

    def finish(part, h, level):
        axis = REDUCE[h][level]
        for copy in state[part][h, level, "both"]:
            copy.wait_recv()
        here = place.on(axis)
        totals = []
        for q in range(2):
            product, _, both1, reduced, _, both2 = buffers[h][q]
            if level == 0:
                total = add(product[part, pl.ds(here * SIDE, SIDE)], both1[part, 0], both1[part, 1])
                reduced[part] = total.astype(jnp.bfloat16)
            else:
                totals.append(add(reduced[part, here], both2[part, 0], both2[part, 1]))
        return totals

    def products(part):
        for at in range(part * POS, (part + 1) * POS):
            if at in lands:
                lands[at].wait_recv()
        rows = arrived[pl.ds(part * POS, POS)].reshape(POS * CAP, features).astype(jnp.float32)
        squares = jnp.sum(rows * rows, axis=1, keepdims=True)
        extra = jnp.broadcast_to(squares, (POS * CAP, EXTRA)).astype(jnp.bfloat16)
        scaled = (rows * gain_ref[...]).astype(jnp.bfloat16)
        for h in range(2):
            for q, matrix in enumerate((gate_ref, up_ref)):
                value = dot(scaled, matrix[:, pl.ds(h * half, half)], NN).astype(jnp.bfloat16)
                value = value.reshape(N_TP, SUB, half)
                product = buffers[h][q][0]
                for t, at in enumerate(torus_order(h)):
                    product[part, at, :, pl.ds(0, half)] = value[t]
                    if h == 0 and q == 0:
                        product[part, at, :, pl.ds(half, EXTRA)] = extra[t * SUB : (t + 1) * SUB]
            relay_out(part, h, 0)

    def activate(part):
        (gate_a, up_a), (gate_b, up_b) = [finish(part, h, 1) for h in range(2)]
        inv = lax.rsqrt(gate_a[:, half : half + 1] * (1.0 / D) + EPS_NORM)
        gather = gathers[part]
        for h, (gate, up) in enumerate(((gate_a[:, :half], up_a), (gate_b, up_b))):
            gate = gate * inv
            value = (gate * sigmoid(gate) * (up * inv)).astype(jnp.bfloat16)
            for q in range(2):
                hidden[h][part, gather.own(h), q] = value[:, q * (half // 2) : (q + 1) * (half // 2)]
            gather.stage(0, h)

    def outputs(part):
        total = jnp.zeros((POS * CAP, features), jnp.float32)
        for h in range(2):
            gathers[part].stage(4, h)
            for q in range(2):
                blocks = [hidden[h][part, at, q] for at in torus_order(h)]
                at = h * half + q * (half // 2)
                total += dot(jnp.concatenate(blocks, axis=0), down_ref[pl.ds(at, half // 2), :], NN)
        results[pl.ds(part * POS, POS)] = total.astype(jnp.bfloat16).reshape(POS, CAP, features)
        for at, there, device in z_peers:
            if part * POS <= at < (part + 1) * POS:
                back[at] = copies(results.at[at], returned.at[there], device)
                back[at].start()
        if part == 0:
            returned[0] = results[0]

    def both(action):
        def run(part):
            for h in range(2):
                action(part, h)
        return run

    stages = [
        products,
        both(lambda part, h: join(part, h, 0)),
        both(lambda part, h: (finish(part, h, 0), relay_out(part, h, 1))),
        both(lambda part, h: join(part, h, 1)),
        activate,
        both(lambda part, h: gathers[part].stage(1, h)),
        both(lambda part, h: gathers[part].stage(2, h)),
        both(lambda part, h: gathers[part].stage(3, h)),
        outputs,
    ]
    begins = (0.0, 5.0, 12.0, 21.0)
    plan = sorted(
        (begins[part] + 3.0 * n, part, n) for part in range(PARTS) for n in range(len(stages))
    )
    for _, part, n in plan:
        stages[n](part)

    came = {there: back[at] for at, there, _ in z_peers}
    total = mid_ref[...].astype(jnp.float32)
    for part in range(PARTS):
        for at in range(part * POS, (part + 1) * POS):
            if at in came:
                came[at].wait_recv()
        rows = returned[pl.ds(part * POS, POS)].reshape(POS * CAP, features)
        columns = pl.ds(part * POS * CAP, POS * CAP)
        total += dot(high_ref[:, columns], rows, NN) + dot(low_ref[:, columns], rows, NN)
    out_ref[...] = total.astype(jnp.bfloat16)
    copies.drain()


def back(midway, norm_gain, pick, high, low, gate, up, down):
    features = midway.shape[1]
    vmem = pl.BlockSpec(memory_space=pltpu.VMEM)
    return pl.pallas_call(
        back_kernel,
        in_specs=[vmem] * 8,
        out_specs=vmem,
        out_shape=jax.ShapeDtypeStruct(midway.shape, jnp.bfloat16),
        scratch_shapes=back_scratch(gate.shape[1], features),
        compiler_params=pltpu.CompilerParams(collective_id=1, has_side_effects=True),
        name="back",
    )(midway, norm_gain.reshape(1, features), pick, high, low, gate, up, down)


def local(
    receptance,
    key_vectors,
    value_vectors,
    decay_logits,
    rate_logits,
    gate_logits,
    group_gain,
    residual,
    mixer_out,
    norm_gain,
    expert_ids,
    route_weight,
    expert_gate,
    expert_up,
    expert_down,
):
    reads, states = mix(receptance, key_vectors, value_vectors, decay_logits, rate_logits)
    pick, high, low = route(expert_ids, route_weight)
    midway = front(reads, states, gate_logits, group_gain, mixer_out, residual)
    return back(midway, norm_gain, pick, high, low, expert_gate[0], expert_up[0], expert_down[0])


def solution(mesh):
    placed = (
        P("sp", "tp"),
        P("sp", "tp"),
        P("sp", "tp"),
        P("sp", "tp"),
        P("sp", "tp"),
        P("sp", "tp"),
        P("tp"),
        P("sp", "tp"),
        P(None, "tp"),
        P("tp"),
        P("sp", None),
        P("sp", None),
        P("sp", "tp", None),
        P("sp", "tp", None),
        P("sp", None, "tp"),
    )
    return jax.shard_map(
        local, mesh=mesh, in_specs=placed, out_specs=P("sp", "tp"), check_vma=False
    )
```

```python
import jax
import jax.numpy as jnp
from jax import lax
from jax.experimental import pallas as pl
from jax.experimental.pallas import tpu as pltpu
from jax.sharding import PartitionSpec as P

D = 4096
HEAD = 64
CHUNK = 128
EXP_HALF = 0.6065306597126334

NZ = 16
N_SP = 2 * NZ
SIDE = 4
N_TP = SIDE * SIDE
CAP = 32
PARTS = 4
POS = N_SP // PARTS
SUB = POS * CAP // N_TP

EPS_GROUP = 0.00064
EPS_NORM = 1e-06
MESH = pl.DeviceIdType.MESH

OFFSETS = [NZ // 2]
for _far in range(NZ // 2 - 1, 0, -1):
    OFFSETS += [_far, -_far]
OFFSETS += [0]
HOME = N_SP - 2
INVERSE = [OFFSETS.index(-o if o != NZ // 2 else o) for o in OFFSETS]


def split(x):
    hi = x.astype(jnp.bfloat16)
    lo = (x - hi.astype(jnp.float32)).astype(jnp.bfloat16)
    return hi, lo


def dot(a, b, dims):
    return lax.dot_general(a, b, (dims, ((), ())), preferred_element_type=jnp.float32)


NN = ((1,), (0,))
NT = ((1,), (1,))
TN = ((0,), (0,))


def dot3(a, b, dims=NN):
    return dot(a[0], b[0], dims) + (dot(a[0], b[1], dims) + dot(a[1], b[0], dims))


def dot2(a, b, dims=NN):
    return dot(a[0], b, dims) + dot(a[1], b, dims)


def sigmoid(x):
    return 1.0 / (1.0 + jnp.exp(-x))


def mix_kernel(r_ref, k_ref, v_ref, d_ref, a_ref, out_ref, state_ref):
    tokens = r_ref.shape[0]
    chunks = tokens // CHUNK
    row = lax.broadcasted_iota(jnp.int32, (CHUNK, CHUNK), 0)
    col = lax.broadcasted_iota(jnp.int32, (CHUNK, CHUNK), 1)
    strict = col < row
    causal = col <= row
    eye = jnp.where(col == row, 1.0, 0.0)
    ones_lower = jnp.where(causal, 1.0, 0.0).astype(jnp.bfloat16)
    low = lax.broadcasted_iota(jnp.int32, (CHUNK, 2 * HEAD), 1) < HEAD

    work = []
    for chunk in range(chunks):
        rows = pl.ds(chunk * CHUNK, CHUNK)
        recept = r_ref[rows, :].astype(jnp.float32)
        keyvec = k_ref[rows, :].astype(jnp.float32)
        logdec = -EXP_HALF * sigmoid(d_ref[rows, :].astype(jnp.float32))
        first, second = split(logdec)
        third = (logdec - first.astype(jnp.float32) - second.astype(jnp.float32)).astype(jnp.bfloat16)
        cum_in = dot(ones_lower, first, NN) + (
            dot(ones_lower, second, NN) + dot(ones_lower, third, NN)
        )
        cum_end = cum_in[CHUNK - 1 :, :]
        squares = keyvec * keyvec
        norms = jnp.where(
            low,
            jnp.sum(squares[:, :HEAD], axis=1, keepdims=True),
            jnp.sum(squares[:, HEAD:], axis=1, keepdims=True),
        )
        unit_key = keyvec * lax.rsqrt(1.0 + norms)
        correction = unit_key * sigmoid(a_ref[rows, :].astype(jnp.float32))
        growth = jnp.exp(-cum_in)
        tail = jnp.exp(cum_end - cum_in)
        r_scaled = recept * jnp.exp(cum_in)
        u_scaled = unit_key * jnp.exp(cum_in - logdec)
        queries = split(jnp.concatenate([u_scaled, r_scaled], axis=0))
        sources = split(jnp.concatenate([keyvec * growth, correction * growth], axis=0))
        tails = split(jnp.concatenate([keyvec * tail, -(correction * tail)], axis=0))
        keep = jnp.broadcast_to(jnp.exp(cum_end), (2 * HEAD, 2 * HEAD)).T
        values = v_ref[rows, :]
        for head in range(2):
            lanes = slice(head * HEAD, (head + 1) * HEAD)
            query = tuple(q[:, lanes] for q in queries)
            source = tuple(s[:, lanes] for s in sources)
            scores = dot3(query, source, NT)
            work.append(
                dict(
                    head=head,
                    chunk=chunk,
                    query=query,
                    tail=tuple(t[:, lanes] for t in tails),
                    keep=keep[lanes, :],
                    value=jnp.concatenate(
                        [values[:, lanes], jnp.zeros((CHUNK, HEAD), jnp.bfloat16)], axis=1
                    ),
                    key_both=split(
                        jnp.concatenate(
                            [
                                jnp.where(strict, scores[:CHUNK, :CHUNK], 0.0),
                                jnp.where(causal, scores[CHUNK:, :CHUNK], 0.0),
                            ],
                            axis=0,
                        )
                    ),
                    pull=jnp.where(strict, scores[:CHUNK, CHUNK:], 0.0),
                    corr_read=split(jnp.where(causal, scores[CHUNK:, CHUNK:], 0.0)),
                )
            )
    for item in work:
        item["inverse"] = eye - jnp.where(row // 2 == col // 2, item["pull"], 0.0)
        item["from_values"] = dot2(item["key_both"], item["value"])
    size = 2
    while size < CHUNK:
        joined = (row // (2 * size) == col // (2 * size)) & (row // size != col // size)
        halves = []
        for item in work:
            inverse = split(item["inverse"])
            between = split(jnp.where(joined, item["pull"], 0.0))
            halves.append((inverse, dot3(between, inverse)))
        for item, (inverse, half) in zip(work, halves):
            item["inverse"] = item["inverse"] - dot3(inverse, split(half))
        size *= 2
    key_row = lax.broadcasted_iota(jnp.int32, (HEAD, 2 * HEAD), 0)
    lane = lax.broadcasted_iota(jnp.int32, (HEAD, 2 * HEAD), 1)
    start = jnp.where(lane == key_row + HEAD, 1.0, 0.0)
    states = [start, start]
    for item in work:
        head = item["head"]
        state = states[head]
        from_start = dot3(item["query"], split(state)) + item["from_values"]
        pulled = dot3(split(item["inverse"]), split(from_start[:CHUNK]))
        pulled_parts = split(pulled)
        out_ref[pl.ds(item["chunk"] * CHUNK, CHUNK), pl.ds(head * 2 * HEAD, 2 * HEAD)] = (
            from_start[CHUNK:] - dot3(item["corr_read"], pulled_parts)
        )
        key_tail = tuple(t[:CHUNK] for t in item["tail"])
        corr_tail = tuple(t[CHUNK:] for t in item["tail"])
        states[head] = (
            item["keep"] * state
            + dot2(key_tail, item["value"], TN)
            + dot3(corr_tail, pulled_parts, TN)
        )
    for head in range(2):
        state_ref[pl.ds(head * HEAD, HEAD), :] = states[head].astype(jnp.bfloat16)


def route(place, ids_ref, weight_ref, pick_ref, high_ref, low_ref):
    tokens = ids_ref.shape[1]
    slots = N_SP * CAP
    expert = lax.broadcasted_iota(jnp.int32, (128, tokens), 0)
    named = [ids_ref[k : k + 1, :] == expert for k in range(2)]
    onehot = jnp.where(named[0] | named[1], 1.0, 0.0).astype(jnp.bfloat16)
    row = lax.broadcasted_iota(jnp.int32, (tokens, tokens), 0)
    col = lax.broadcasted_iota(jnp.int32, (tokens, tokens), 1)
    before = jnp.where(row < col, 1.0, 0.0).astype(jnp.bfloat16)
    earlier = dot(onehot, before, NN).astype(jnp.bfloat16)
    weight = jnp.where(named[0], weight_ref[0:1, :], 0.0) + jnp.where(named[1], weight_ref[1:2, :], 0.0)
    high, low = split(weight)
    slot = lax.broadcasted_iota(jnp.int32, (slots, 128), 0)
    source = lax.broadcasted_iota(jnp.int32, (slots, 128), 1)
    near = slot // (2 * CAP)
    step = NZ // 2 - (near + 1) // 2
    off = jnp.where(near % 2 == 1, step, NZ - step)
    chip = (place.z + off) % NZ
    core = (place.core + slot // CAP) % 2
    spread = jnp.where(source == chip * 2 + core, 1.0, 0.0).astype(jnp.bfloat16)
    rank = (lax.broadcasted_iota(jnp.int32, (slots, tokens), 0) % CAP).astype(jnp.float32)
    taken = jnp.where(dot(spread, earlier, NN) == rank, dot(spread, onehot, NN), 0.0)
    pick_ref[...] = taken.astype(jnp.bfloat16)
    high_ref[...] = (taken * dot(spread, high, NN)).astype(jnp.bfloat16)
    low_ref[...] = (taken * dot(spread, low, NN)).astype(jnp.bfloat16)


class Place:
    def __init__(self):
        self.sp = lax.axis_index("sp")
        self.tp = lax.axis_index("tp")
        self.z, self.core = self.sp // 2, self.sp % 2
        self.y, self.x = self.tp // SIDE, self.tp % SIDE

    def chip(self, off, other=False):
        core = (self.core + 1) % 2 if other else self.core
        return ((self.z + off + NZ) % NZ) * 2 + core

    def at_z(self, off, other=False):
        return {"sp": self.chip(off, other), "tp": self.tp}

    def along(self, axis, off):
        if axis == "x":
            return {"sp": self.sp, "tp": self.y * SIDE + (self.x + off + SIDE) % SIDE}
        return {"sp": self.sp, "tp": ((self.y + off + SIDE) % SIDE) * SIDE + self.x}

    def on(self, axis, off=0):
        return ((self.x if axis == "x" else self.y) + off + SIDE) % SIDE


class Copies:
    def __init__(self, send, recv):
        self.send, self.recv = send, recv
        self.made = []

    def __call__(self, src, dst, device):
        index = len(self.made)
        copy = pltpu.make_async_remote_copy(
            src_ref=src,
            dst_ref=dst,
            send_sem=self.send.at[index],
            recv_sem=self.recv.at[index],
            device_id=device,
            device_id_type=MESH,
        )
        self.made.append(copy)
        return copy

    def drain(self):
        for copy in self.made:
            copy.wait_send()


ORDER = (("x", "y"), ("y", "x"))


class TorusGather:
    def __init__(self, place, copies, blocks):
        self.place, self.copies, self.blocks = place, copies, blocks
        self.state = [dict() for _ in blocks]

    def own(self, h):
        first, second = ORDER[h]
        return self.place.on(second) * SIDE + self.place.on(first)

    def exchange(self, h, axis, mine):
        up, down = self.place.along(axis, 1), self.place.along(axis, -1)
        whole = mine(0)
        direct = [self.copies(whole, whole, up), self.copies(whole, whole, down)]
        for copy in direct:
            copy.start()
        return direct, up, down

    def relay(self, direct, up, down, mine, half):
        passed = []
        for side, (copy, off, target) in enumerate(zip(direct, (-1, 1), (up, down))):
            copy.wait_recv()
            piece = half(mine(off), side)
            passed.append(self.copies(piece, piece, target))
            passed[-1].start()
        return passed

    def stage(self, n, h):
        first, second = ORDER[h]
        place, block, s = self.place, self.blocks[h], self.state[h]

        def one(off):
            return block.at[place.on(second) * SIDE + place.on(first, off)]

        def four(off):
            return block.at[pl.ds(place.on(second, off) * SIDE, SIDE)]

        if n == 0:
            s["a"] = [self.copies(one(0), one(0), place.along(first, off)) for off in (2, 1, -1)]
            for copy in s["a"]:
                copy.start()
        elif n == 1:
            for copy in s["a"]:
                copy.wait_recv()
            s["c"] = self.exchange(h, second, four)
        elif n == 2:
            s["d"] = self.relay(*s["c"], four, lambda ref, side: ref.at[:, side])
        else:
            for copy in s["d"]:
                copy.wait_recv()


def torus_order(h):
    if h == 0:
        return list(range(N_TP))
    return [x * SIDE + y for y in range(SIDE) for x in range(SIDE)]


def front(
    place, copies, meanwhile,
    reads_ref, states_ref, gate_ref, gain_ref, weight_ref, residual_ref, out_ref, maps, halves,
):
    partner = place.at_z(0, True)
    up, down = place.at_z(1), place.at_z(-1)
    tokens = out_ref.shape[0]
    pieces = 2
    rows = states_ref.shape[0] // pieces
    maps[place.sp] = states_ref[...]

    def slot(off):
        return place.chip(off)

    def hop(n, direction, piece):
        part = pl.ds(piece * rows, rows)
        target = up if direction > 0 else down
        here = slot(-direction * (n - 1))
        src = states_ref.at[part] if n == 1 else maps.at[here, part]
        copy = copies(src, maps.at[here, part], target)
        copy.start()
        return copy

    across = [copies(states_ref, maps.at[slot(0)], partner)]
    last = {1: NZ // 2, -1: NZ // 2 - 1}
    current = {}
    for piece in range(pieces):
        for direction in (1, -1):
            current[direction, piece] = hop(1, direction, piece)
    across[0].start()
    meanwhile()
    for n in range(1, NZ // 2 + 1):
        for piece in range(pieces):
            for direction in (1, -1):
                if n > last[direction]:
                    continue
                current[direction, piece].wait_recv()
                if n < last[direction]:
                    current[direction, piece] = hop(n + 1, direction, piece)
        for direction in (1, -1):
            if n <= last[direction]:
                here = slot(-direction * n)
                copy = copies(maps.at[here], maps.at[here], partner)
                copy.start()
                across.append(copy)
    for copy in across:
        copy.wait_recv()

    heads = states_ref.shape[0] // HEAD

    def fold(step, carried):
        following = []
        for head in range(heads):
            both = maps[step, pl.ds(head * HEAD, HEAD), :]
            hi, lo = split(carried[head])
            step_map = both[:, HEAD:]
            following.append(
                both[:, :HEAD].astype(jnp.float32) + dot(step_map, hi, NN) + dot(step_map, lo, NN)
            )
        return tuple(following)

    zero = jnp.zeros((HEAD, HEAD), jnp.float32)
    incoming = lax.fori_loop(0, place.sp, fold, (zero,) * heads)
    scaled = []
    for head in range(heads):
        both = reads_ref[:, pl.ds(head * 2 * HEAD, 2 * HEAD)]
        state_read = both[:, :HEAD] + dot3(split(both[:, HEAD:]), split(incoming[head]))
        centred = state_read - jnp.mean(state_read, axis=1, keepdims=True)
        variance = jnp.mean(centred * centred, axis=1, keepdims=True)
        scaled.append(centred * lax.rsqrt(variance + EPS_GROUP))
    gated = (
        jnp.concatenate(scaled, axis=1)
        * gain_ref[...]
        * sigmoid(gate_ref[...].astype(jnp.float32))
    ).astype(jnp.bfloat16)
    gather = TorusGather(place, copies, halves)
    quarter = tokens // 4
    for h in range(2):
        for q in range(2):
            at = (2 * h + q) * quarter
            halves[h][gather.own(h), q] = gated[at : at + quarter]
    for n in range(4):
        for h in range(2):
            gather.stage(n, h)
    width = gated.shape[1]
    for h in range(2):
        total = jnp.zeros((tokens // 2, out_ref.shape[1]), jnp.float32)
        for t, at in enumerate(torus_order(h)):
            block = halves[h][at].reshape(tokens // 2, width)
            total += dot(block, weight_ref[pl.ds(t * width, width), :], NN)
        part = pl.ds(h * (tokens // 2), tokens // 2)
        out_ref[part, :] = (residual_ref[part, :].astype(jnp.float32) + total).astype(jnp.bfloat16)


EXTRA = 128


def widths(ff):
    return ((ff // 2 + EXTRA, ff // 2), (ff // 2, ff // 2))


def back_scratch(ff, features):
    wide = widths(ff)
    per_part = []
    for h in range(2):
        for q in range(2):
            w = wide[h][q]
            per_part += [
                pltpu.VMEM((PARTS, N_TP, SUB, w), jnp.bfloat16),
                pltpu.VMEM((PARTS, SIDE, SUB, w), jnp.bfloat16),
                pltpu.VMEM((PARTS, 2, SIDE, SUB, w), jnp.bfloat16),
                pltpu.VMEM((PARTS, SIDE, SUB, w), jnp.bfloat16),
                pltpu.VMEM((PARTS, 3, SUB, w), jnp.bfloat16),
            ]
    hidden = [pltpu.VMEM((PARTS, N_TP, 2, SUB, ff // 4), jnp.bfloat16) for _ in range(2)]
    slots = [pltpu.VMEM((N_SP, CAP, features), jnp.bfloat16) for _ in range(4)]
    return slots + hidden + per_part


REDUCE = (("y", "x"), ("x", "y"))


def peers_along_z(place):
    return [
        (2 * near + other, 2 * INVERSE[near] + other, place.at_z(off, bool(other)))
        for near, off in enumerate(OFFSETS)
        for other in range(2)
        if off != 0 or other
    ]


def back(
    place, copies,
    mid_ref, gain_ref, pick_ref, high_ref, low_ref, gate_ref, up_ref, down_ref, out_ref, scratch,
):
    outgoing, arrived, results, returned = scratch[:4]
    hidden = scratch[4:6]
    buffers = [[scratch[6 + (2 * h + q) * 5 : 11 + (2 * h + q) * 5] for q in range(2)] for h in range(2)]
    features = mid_ref.shape[1]
    ff = gate_ref.shape[1]
    half = ff // 2
    z_peers = peers_along_z(place)
    for part in range(PARTS):
        rows = pl.ds(part * POS * CAP, POS * CAP)
        outgoing[pl.ds(part * POS, POS)] = (
            dot(pick_ref[rows, :], mid_ref[...], NN).astype(jnp.bfloat16).reshape(POS, CAP, features)
        )
    arrived[HOME] = outgoing[HOME]
    dispatch = {}
    for at, there, device in z_peers:
        dispatch[at] = copies(outgoing.at[at], arrived.at[there], device)
        dispatch[at].start()
    lands = {there: dispatch[at] for at, there, _ in z_peers}
    back = {}
    state = [dict() for _ in range(PARTS)]
    gathers = [
        TorusGather(place, copies, [hidden[h].at[part] for h in range(2)]) for part in range(PARTS)
    ]

    def add(*refs):
        total = refs[0].astype(jnp.float32)
        for ref in refs[1:]:
            total += ref.astype(jnp.float32)
        return total

    def relay_out(part, h):
        axis = REDUCE[h][0]
        far = pl.ds(place.on(axis, 2) * SIDE, SIDE)
        sent = []
        for q, off in ((0, 1), (1, -1)):
            product, passed = buffers[h][q][:2]
            copy = copies(product.at[part, far], passed.at[part], place.along(axis, off))
            copy.start()
            sent.append(copy)
        state[part][h, "relay"] = sent

    def join(part, h):
        axis = REDUCE[h][0]
        sent = []
        for side, off in ((0, 1), (1, -1)):
            state[part][h, "relay"][side].wait_recv()
            near = pl.ds(place.on(axis, off) * SIDE, SIDE)
            for q in (1 - side, side):
                product, passed, both = buffers[h][q][:3]
                if q == side:
                    product[part, near] = add(product[part, near], passed[part]).astype(jnp.bfloat16)
                copy = copies(product.at[part, near], both.at[part, side], place.along(axis, off))
                copy.start()
                sent.append(copy)
        state[part][h, "both"] = sent

    def halfway(part, h):
        first, second = REDUCE[h]
        for copy in state[part][h, "both"]:
            copy.wait_recv()
        here = pl.ds(place.on(first) * SIDE, SIDE)
        sent = []
        for q in range(2):
            product, _, both, reduced, others = buffers[h][q]
            total = add(product[part, here], both[part, 0], both[part, 1])
            reduced[part] = total.astype(jnp.bfloat16)
            for side, off in enumerate((2, 1, -1)):
                copy = copies(
                    reduced.at[part, place.on(second, off)],
                    others.at[part, side],
                    place.along(second, off),
                )
                copy.start()
                sent.append(copy)
        state[part][h, "others"] = sent

    def finish(part, h):
        second = REDUCE[h][1]
        for copy in state[part][h, "others"]:
            copy.wait_recv()
        return [
            add(reduced[part, place.on(second)], *[others[part, side] for side in range(3)])
            for _, _, _, reduced, others in buffers[h]
        ]

    def products(part):
        for at in range(part * POS, (part + 1) * POS):
            if at in lands:
                lands[at].wait_recv()
        rows = arrived[pl.ds(part * POS, POS)].reshape(POS * CAP, features).astype(jnp.float32)
        squares = jnp.sum(rows * rows, axis=1, keepdims=True)
        extra = jnp.broadcast_to(squares, (POS * CAP, EXTRA)).astype(jnp.bfloat16)
        scaled = (rows * gain_ref[...]).astype(jnp.bfloat16)
        for h in range(2):
            for q, matrix in enumerate((gate_ref, up_ref)):
                value = dot(scaled, matrix[:, pl.ds(h * half, half)], NN).astype(jnp.bfloat16)
                value = value.reshape(N_TP, SUB, half)
                product = buffers[h][q][0]
                for t, at in enumerate(torus_order(h)):
                    product[part, at, :, pl.ds(0, half)] = value[t]
                    if h == 0 and q == 0:
                        product[part, at, :, pl.ds(half, EXTRA)] = extra[t * SUB : (t + 1) * SUB]
            relay_out(part, h)

    def activate(part):
        (gate_a, up_a), (gate_b, up_b) = [finish(part, h) for h in range(2)]
        inv = lax.rsqrt(gate_a[:, half : half + 1] * (1.0 / D) + EPS_NORM)
        gather = gathers[part]
        for h, (gate, up) in enumerate(((gate_a[:, :half], up_a), (gate_b, up_b))):
            gate = gate * inv
            value = (gate * sigmoid(gate) * (up * inv)).astype(jnp.bfloat16)
            for q in range(2):
                hidden[h][part, gather.own(h), q] = value[:, q * (half // 2) : (q + 1) * (half // 2)]
            gather.stage(0, h)

    def outputs(part):
        total = jnp.zeros((POS * CAP, features), jnp.float32)
        for h in range(2):
            gathers[part].stage(3, h)
            for q in range(2):
                blocks = [hidden[h][part, at, q] for at in torus_order(h)]
                at = h * half + q * (half // 2)
                total += dot(jnp.concatenate(blocks, axis=0), down_ref[pl.ds(at, half // 2), :], NN)
        results[pl.ds(part * POS, POS)] = total.astype(jnp.bfloat16).reshape(POS, CAP, features)
        for at, there, device in z_peers:
            if part * POS <= at < (part + 1) * POS:
                back[at] = copies(results.at[at], returned.at[there], device)
                back[at].start()
        if part == HOME // POS:
            returned[HOME] = results[HOME]

    def both(action):
        def run(part):
            for h in range(2):
                action(part, h)
        return run

    stages = [
        products,
        both(join),
        both(halfway),
        activate,
        both(lambda part, h: gathers[part].stage(1, h)),
        both(lambda part, h: gathers[part].stage(2, h)),
        outputs,
    ]
    begins = (0.0, 7.0, 11.0, 13.0)
    plan = sorted(
        (begins[part] + 3.0 * n, part, n) for part in range(PARTS) for n in range(len(stages))
    )
    for _, part, n in plan:
        stages[n](part)

    came = {there: back[at] for at, there, _ in z_peers}
    total = mid_ref[...].astype(jnp.float32)
    for part in range(PARTS):
        for at in range(part * POS, (part + 1) * POS):
            if at in came:
                came[at].wait_recv()
        rows = returned[pl.ds(part * POS, POS)].reshape(POS * CAP, features)
        columns = pl.ds(part * POS * CAP, POS * CAP)
        total += dot(high_ref[columns, :], rows, TN) + dot(low_ref[columns, :], rows, TN)
    out_ref[...] = total.astype(jnp.bfloat16)


def kernel(
    r_ref, k_ref, v_ref, d_ref, a_ref, gate_logits_ref, group_gain_ref, residual_ref, norm_gain_ref,
    ids_ref, route_weight_ref, mixer_hbm, gate_hbm, up_hbm, down_hbm, out_ref, *scratch
):
    mixer, gate, up, down, loaded, send, recv = scratch[:7]
    reads, states, pick, high, low, midway, maps = scratch[7:14]
    halves = scratch[14:16]
    place = Place()
    copies = Copies(send, recv)
    barrier = pltpu.get_barrier_semaphore()
    others = [peer[2] for peer in peers_along_z(place)]
    others += [place.along(axis, off) for axis in "xy" for off in (2, 1, -1)]
    for device in others:
        pl.semaphore_signal(barrier, inc=1, device_id=device, device_id_type=MESH)
    loads = [
        pltpu.make_async_copy(src, dst, loaded.at[n])
        for n, (src, dst) in enumerate(
            [(mixer_hbm, mixer), (gate_hbm, gate), (up_hbm, up), (down_hbm, down)]
        )
    ]
    for load in loads:
        load.start()
    for pair in range(r_ref.shape[1] // (2 * HEAD)):
        lanes = pl.ds(pair * 2 * HEAD, 2 * HEAD)
        mix_kernel(
            *[ref.at[:, lanes] for ref in (r_ref, k_ref, v_ref, d_ref, a_ref)],
            reads.at[:, pl.ds(pair * 4 * HEAD, 4 * HEAD)],
            states.at[lanes, :],
        )
    pl.semaphore_wait(barrier, len(others))

    def meanwhile():
        route(place, ids_ref, route_weight_ref, pick, high, low)
        for load in loads:
            load.wait()

    front(
        place, copies, meanwhile,
        reads, states, gate_logits_ref, group_gain_ref, mixer, residual_ref, midway, maps, halves,
    )
    back(
        place, copies,
        midway, norm_gain_ref, pick, high, low, gate, up, down, out_ref, scratch[16:],
    )
    copies.drain()


def local(
    receptance,
    key_vectors,
    value_vectors,
    decay_logits,
    rate_logits,
    gate_logits,
    group_gain,
    residual,
    mixer_out,
    norm_gain,
    expert_ids,
    route_weight,
    expert_gate,
    expert_up,
    expert_down,
):
    tokens, channels = residual.shape
    features = norm_gain.shape[0]
    ff = expert_gate.shape[2]
    slots = N_SP * CAP
    count = 64 + 2 * (N_SP - 1) + PARTS * 40
    bf16 = jnp.bfloat16
    vmem = pl.BlockSpec(memory_space=pltpu.VMEM)
    hbm = pl.BlockSpec(memory_space=pl.ANY)
    weights = (mixer_out, expert_gate[0], expert_up[0], expert_down[0])
    return pl.pallas_call(
        kernel,
        in_specs=[vmem] * 11 + [hbm] * 4,
        out_specs=vmem,
        out_shape=jax.ShapeDtypeStruct((tokens, features), bf16),
        scratch_shapes=[pltpu.VMEM(w.shape, bf16) for w in weights]
        + [
            pltpu.SemaphoreType.DMA((len(weights),)),
            pltpu.SemaphoreType.DMA((count,)),
            pltpu.SemaphoreType.DMA((count,)),
            pltpu.VMEM((tokens, 2 * channels), jnp.float32),
            pltpu.VMEM((channels, 2 * HEAD), bf16),
            pltpu.VMEM((slots, tokens), bf16),
            pltpu.VMEM((slots, tokens), bf16),
            pltpu.VMEM((slots, tokens), bf16),
            pltpu.VMEM((tokens, features), bf16),
            pltpu.VMEM((N_SP, channels, 2 * HEAD), bf16),
            pltpu.VMEM((N_TP, 2, tokens // 4, channels), bf16),
            pltpu.VMEM((N_TP, 2, tokens // 4, channels), bf16),
        ]
        + back_scratch(ff, features),
        compiler_params=pltpu.CompilerParams(
            collective_id=0, has_side_effects=True, vmem_limit_bytes=60 * 1024 * 1024
        ),
        name="layer",
    )(
        receptance, key_vectors, value_vectors, decay_logits, rate_logits, gate_logits,
        group_gain.reshape(1, channels), residual, norm_gain.reshape(1, features),
        expert_ids.T, route_weight.T, *weights,
    )


def solution(mesh):
    placed = (
        P("sp", "tp"),
        P("sp", "tp"),
        P("sp", "tp"),
        P("sp", "tp"),
        P("sp", "tp"),
        P("sp", "tp"),
        P("tp"),
        P("sp", "tp"),
        P(None, "tp"),
        P("tp"),
        P("sp", None),
        P("sp", None),
        P("sp", "tp", None),
        P("sp", "tp", None),
        P("sp", None, "tp"),
    )
    return jax.shard_map(
        local, mesh=mesh, in_specs=placed, out_specs=P("sp", "tp"), check_vma=False
    )
```

```python
import jax
import jax.numpy as jnp
from jax import lax
from jax.experimental import pallas as pl
from jax.experimental.pallas import tpu as pltpu
from jax.sharding import PartitionSpec as P

D = 4096
HEAD = 64
CHUNK = 128
EXP_HALF = 0.6065306597126334

NZ = 16
N_SP = 2 * NZ
SIDE = 4
N_TP = SIDE * SIDE
CAP = 32
PARTS = 4
POS = N_SP // PARTS
SUB = POS * CAP // 8

EPS_GROUP = 0.00064
EPS_NORM = 1e-06
MESH = pl.DeviceIdType.MESH

OFFSETS = [NZ // 2]
for _far in range(NZ // 2 - 1, 0, -1):
    OFFSETS += [_far, -_far]
OFFSETS += [0]
HOME = N_SP - 2
INVERSE = [OFFSETS.index(-o if o != NZ // 2 else o) for o in OFFSETS]


def split(x):
    hi = x.astype(jnp.bfloat16)
    lo = (x - hi.astype(jnp.float32)).astype(jnp.bfloat16)
    return hi, lo


def dot(a, b, dims):
    return lax.dot_general(a, b, (dims, ((), ())), preferred_element_type=jnp.float32)


NN = ((1,), (0,))
NT = ((1,), (1,))
TN = ((0,), (0,))


def dot3(a, b, dims=NN):
    return dot(a[0], b[0], dims) + (dot(a[0], b[1], dims) + dot(a[1], b[0], dims))


def dot2(a, b, dims=NN):
    return dot(a[0], b, dims) + dot(a[1], b, dims)


def sigmoid(x):
    return 1.0 / (1.0 + jnp.exp(-x))


def mix_kernel(r_ref, k_ref, v_ref, d_ref, a_ref, out_ref, state_ref):
    tokens = r_ref.shape[0]
    chunks = tokens // CHUNK
    row = lax.broadcasted_iota(jnp.int32, (CHUNK, CHUNK), 0)
    col = lax.broadcasted_iota(jnp.int32, (CHUNK, CHUNK), 1)
    strict = col < row
    causal = col <= row
    eye = jnp.where(col == row, 1.0, 0.0)
    ones_lower = jnp.where(causal, 1.0, 0.0).astype(jnp.bfloat16)
    low = lax.broadcasted_iota(jnp.int32, (CHUNK, 2 * HEAD), 1) < HEAD

    work = []
    for chunk in range(chunks):
        rows = pl.ds(chunk * CHUNK, CHUNK)
        recept = r_ref[rows, :].astype(jnp.float32)
        keyvec = k_ref[rows, :].astype(jnp.float32)
        logdec = -EXP_HALF * sigmoid(d_ref[rows, :].astype(jnp.float32))
        first, second = split(logdec)
        third = (logdec - first.astype(jnp.float32) - second.astype(jnp.float32)).astype(jnp.bfloat16)
        cum_in = dot(ones_lower, first, NN) + (
            dot(ones_lower, second, NN) + dot(ones_lower, third, NN)
        )
        cum_end = cum_in[CHUNK - 1 :, :]
        squares = keyvec * keyvec
        norms = jnp.where(
            low,
            jnp.sum(squares[:, :HEAD], axis=1, keepdims=True),
            jnp.sum(squares[:, HEAD:], axis=1, keepdims=True),
        )
        unit_key = keyvec * lax.rsqrt(1.0 + norms)
        correction = unit_key * sigmoid(a_ref[rows, :].astype(jnp.float32))
        growth = jnp.exp(-cum_in)
        tail = jnp.exp(cum_end - cum_in)
        r_scaled = recept * jnp.exp(cum_in)
        u_scaled = unit_key * jnp.exp(cum_in - logdec)
        queries = split(jnp.concatenate([u_scaled, r_scaled], axis=0))
        sources = split(jnp.concatenate([keyvec * growth, correction * growth], axis=0))
        tails = split(jnp.concatenate([keyvec * tail, -(correction * tail)], axis=0))
        keep = jnp.broadcast_to(jnp.exp(cum_end), (2 * HEAD, 2 * HEAD)).T
        values = v_ref[rows, :]
        for head in range(2):
            lanes = slice(head * HEAD, (head + 1) * HEAD)
            query = tuple(q[:, lanes] for q in queries)
            source = tuple(s[:, lanes] for s in sources)
            scores = dot3(query, source, NT)
            work.append(
                dict(
                    head=head,
                    chunk=chunk,
                    query=query,
                    tail=tuple(t[:, lanes] for t in tails),
                    keep=keep[lanes, :],
                    value=jnp.concatenate(
                        [values[:, lanes], jnp.zeros((CHUNK, HEAD), jnp.bfloat16)], axis=1
                    ),
                    key_both=split(
                        jnp.concatenate(
                            [
                                jnp.where(strict, scores[:CHUNK, :CHUNK], 0.0),
                                jnp.where(causal, scores[CHUNK:, :CHUNK], 0.0),
                            ],
                            axis=0,
                        )
                    ),
                    pull=jnp.where(strict, scores[:CHUNK, CHUNK:], 0.0),
                    corr_read=split(jnp.where(causal, scores[CHUNK:, CHUNK:], 0.0)),
                )
            )
    for item in work:
        item["inverse"] = eye - jnp.where(row // 2 == col // 2, item["pull"], 0.0)
        item["from_values"] = dot2(item["key_both"], item["value"])
    size = 2
    while size < CHUNK:
        joined = (row // (2 * size) == col // (2 * size)) & (row // size != col // size)
        halves = []
        for item in work:
            inverse = split(item["inverse"])
            between = split(jnp.where(joined, item["pull"], 0.0))
            halves.append((inverse, dot3(between, inverse)))
        for item, (inverse, half) in zip(work, halves):
            item["inverse"] = item["inverse"] - dot3(inverse, split(half))
        size *= 2
    key_row = lax.broadcasted_iota(jnp.int32, (HEAD, 2 * HEAD), 0)
    lane = lax.broadcasted_iota(jnp.int32, (HEAD, 2 * HEAD), 1)
    start = jnp.where(lane == key_row + HEAD, 1.0, 0.0)
    states = [start, start]
    for item in work:
        head = item["head"]
        state = states[head]
        from_start = dot3(item["query"], split(state)) + item["from_values"]
        pulled = dot3(split(item["inverse"]), split(from_start[:CHUNK]))
        pulled_parts = split(pulled)
        out_ref[pl.ds(item["chunk"] * CHUNK, CHUNK), pl.ds(head * 2 * HEAD, 2 * HEAD)] = (
            from_start[CHUNK:] - dot3(item["corr_read"], pulled_parts)
        )
        key_tail = tuple(t[:CHUNK] for t in item["tail"])
        corr_tail = tuple(t[CHUNK:] for t in item["tail"])
        states[head] = (
            item["keep"] * state
            + dot2(key_tail, item["value"], TN)
            + dot3(corr_tail, pulled_parts, TN)
        )
    for head in range(2):
        state_ref[pl.ds(head * HEAD, HEAD), :] = states[head].astype(jnp.bfloat16)


def route(place, ids_ref, weight_ref, pick_ref, high_ref, low_ref):
    tokens = ids_ref.shape[1]
    slots = N_SP * CAP
    expert = lax.broadcasted_iota(jnp.int32, (128, tokens), 0)
    named = [ids_ref[k : k + 1, :] == expert for k in range(2)]
    onehot = jnp.where(named[0] | named[1], 1.0, 0.0).astype(jnp.bfloat16)
    row = lax.broadcasted_iota(jnp.int32, (tokens, tokens), 0)
    col = lax.broadcasted_iota(jnp.int32, (tokens, tokens), 1)
    before = jnp.where(row < col, 1.0, 0.0).astype(jnp.bfloat16)
    earlier = dot(onehot, before, NN).astype(jnp.bfloat16)
    weight = jnp.where(named[0], weight_ref[0:1, :], 0.0) + jnp.where(named[1], weight_ref[1:2, :], 0.0)
    high, low = split(weight)
    slot = lax.broadcasted_iota(jnp.int32, (slots, 128), 0)
    source = lax.broadcasted_iota(jnp.int32, (slots, 128), 1)
    near = slot // (2 * CAP)
    step = NZ // 2 - (near + 1) // 2
    off = jnp.where(near % 2 == 1, step, NZ - step)
    chip = (place.z + off) % NZ
    core = (place.core + slot // CAP) % 2
    spread = jnp.where(source == chip * 2 + core, 1.0, 0.0).astype(jnp.bfloat16)
    rank = (lax.broadcasted_iota(jnp.int32, (slots, tokens), 0) % CAP).astype(jnp.float32)
    taken = jnp.where(dot(spread, earlier, NN) == rank, dot(spread, onehot, NN), 0.0)
    pick_ref[...] = taken.astype(jnp.bfloat16)
    high_ref[...] = (taken * dot(spread, high, NN)).astype(jnp.bfloat16)
    low_ref[...] = (taken * dot(spread, low, NN)).astype(jnp.bfloat16)


class Place:
    def __init__(self):
        self.sp = lax.axis_index("sp")
        self.tp = lax.axis_index("tp")
        self.z, self.core = self.sp // 2, self.sp % 2
        self.y, self.x = self.tp // SIDE, self.tp % SIDE

    def chip(self, off, other=False):
        core = (self.core + 1) % 2 if other else self.core
        return ((self.z + off + NZ) % NZ) * 2 + core

    def at_z(self, off, other=False):
        return {"sp": self.chip(off, other), "tp": self.tp}

    def along(self, axis, off):
        if axis == "x":
            return {"sp": self.sp, "tp": self.y * SIDE + (self.x + off + SIDE) % SIDE}
        return {"sp": self.sp, "tp": ((self.y + off + SIDE) % SIDE) * SIDE + self.x}

    def on(self, axis, off=0):
        return ((self.x if axis == "x" else self.y) + off + SIDE) % SIDE


class Copies:
    def __init__(self, send, recv):
        self.send, self.recv = send, recv
        self.made = []

    def __call__(self, src, dst, device):
        index = len(self.made)
        copy = pltpu.make_async_remote_copy(
            src_ref=src,
            dst_ref=dst,
            send_sem=self.send.at[index],
            recv_sem=self.recv.at[index],
            device_id=device,
            device_id_type=MESH,
        )
        self.made.append(copy)
        return copy

    def drain(self):
        for copy in self.made:
            copy.wait_send()


ORDER = (("x", "y"), ("y", "x"))


class TorusGather:
    def __init__(self, place, copies, blocks):
        self.place, self.copies, self.blocks = place, copies, blocks
        self.state = [dict() for _ in blocks]

    def at(self, h, first=0, second=0):
        one, two = ORDER[h]
        return self.place.on(two, second) * SIDE + self.place.on(one, first)

    def block(self, h, first=0, second=0):
        return self.blocks[h].at[self.at(h, first, second)]

    def row(self, h, second=0):
        start = self.place.on(ORDER[h][1], second) * SIDE
        return self.blocks[h].at[pl.ds(start, SIDE)]

    def begin(self, h):
        mine = self.block(h)
        sent = {off: self.copies(mine, mine, self.place.along(ORDER[h][0], off)) for off in (2, 1, -1)}
        for copy in sent.values():
            copy.start()
        self.state[h]["first"] = sent

    def arrive(self, h, off):
        self.state[h]["first"][off].wait_recv()

    def pair(self, h, ref):
        sent = [self.copies(ref, ref, self.place.along(ORDER[h][1], off)) for off in (1, -1)]
        for copy in sent:
            copy.start()
        return sent

    def relay(self, h, sent, ref_of, half):
        passed = []
        for side, (copy, off) in enumerate(zip(sent, (1, -1))):
            copy.wait_recv()
            piece = half(ref_of(-off), side)
            passed.append(self.copies(piece, piece, self.place.along(ORDER[h][1], off)))
            passed[-1].start()
        return passed


def front(
    place, copies, meanwhile,
    reads_ref, states_ref, gate_ref, gain_ref, weight_ref, residual_ref, out_ref,
    cores, maps, incoming_ref, halves,
):
    partner = place.at_z(0, True)
    tokens = out_ref.shape[0]
    heads = states_ref.shape[0] // HEAD
    mine = heads // 2
    cores[place.core] = states_ref[...]
    swap = copies(states_ref, cores.at[place.core], partner)
    swap.start()
    swap.wait_recv()
    for head in range(mine):
        rows = pl.ds(pl.multiple_of((place.core * mine + head) * HEAD, HEAD), HEAD)
        later = cores[1, rows, :]
        added = dot(later[:, HEAD:], cores[0, rows, :], NN)
        state = later[:, :HEAD].astype(jnp.float32) + added[:, :HEAD]
        maps[place.z, pl.ds(head * HEAD, HEAD), :] = jnp.concatenate(
            [state, added[:, HEAD:]], axis=1
        ).astype(jnp.bfloat16)

    came = {}
    last = {1: NZ // 2, -1: NZ // 2 - 1}

    def pass_on(direction, d):
        ref = maps.at[(place.z - direction * d + NZ) % NZ]
        for far in (2, 1):
            if d + far <= last[direction]:
                came[direction, d + far] = copies(ref, ref, place.at_z(direction * far))
                came[direction, d + far].start()

    for d in range(0, NZ // 2, 2):
        for direction in (1, -1):
            if d:
                came[direction, d].wait_recv()
            pass_on(direction, d)
        if d // 2 < len(meanwhile):
            meanwhile[d // 2]()
    for direction in (1, -1):
        for d in range(1, last[direction] + 1):
            if d % 2 or d == NZ // 2:
                came[direction, d].wait_recv()

    def fold(step, carried):
        following = []
        for head in range(mine):
            both = maps[step, pl.ds(head * HEAD, HEAD), :]
            hi, lo = split(carried[head])
            step_map = both[:, HEAD:]
            following.append(
                both[:, :HEAD].astype(jnp.float32) + dot(step_map, hi, NN) + dot(step_map, lo, NN)
            )
        return tuple(following)

    zero = jnp.zeros((HEAD, HEAD), jnp.float32)
    incoming_ref[place.core] = jnp.concatenate(
        lax.fori_loop(0, place.z, fold, (zero,) * mine), axis=1
    )
    swap = copies(incoming_ref.at[place.core], incoming_ref.at[place.core], partner)
    swap.start()
    second = (jnp.zeros((HEAD, HEAD), jnp.int32) + place.core) == 1
    swap.wait_recv()
    scaled = []
    for head in range(heads):
        before = incoming_ref[head // mine, :, (head % mine) * HEAD : (head % mine + 1) * HEAD]
        both = cores[0, pl.ds(head * HEAD, HEAD), :]
        hi, lo = split(before)
        step_map = both[:, HEAD:]
        after = both[:, :HEAD].astype(jnp.float32) + dot(step_map, hi, NN) + dot(step_map, lo, NN)
        state = jnp.where(second, after, before)
        both = reads_ref[:, pl.ds(head * 2 * HEAD, 2 * HEAD)]
        state_read = both[:, :HEAD] + dot3(split(both[:, HEAD:]), split(state))
        centred = state_read - jnp.mean(state_read, axis=1, keepdims=True)
        variance = jnp.mean(centred * centred, axis=1, keepdims=True)
        scaled.append(centred * lax.rsqrt(variance + EPS_GROUP))
    gated = (
        jnp.concatenate(scaled, axis=1)
        * gain_ref[...]
        * sigmoid(gate_ref[...].astype(jnp.float32))
    ).astype(jnp.bfloat16)
    gather = TorusGather(place, copies, halves)
    quarter = tokens // 4
    for h in range(2):
        for q in range(2):
            at = (2 * h + q) * quarter
            halves[h][gather.at(h), q] = gated[at : at + quarter]
    width = gated.shape[1]
    totals = [jnp.zeros((tokens // 2, out_ref.shape[1]), jnp.float32) for _ in range(2)]

    def project(h, first, second):
        x, y = (first, second) if h == 0 else (second, first)
        t = place.on("y", y) * SIDE + place.on("x", x)
        rows = pl.ds(pl.multiple_of(t * width, width), width)
        block = halves[h][gather.at(h, first, second)].reshape(tokens // 2, width)
        totals[h] += dot(block, weight_ref[rows, :], NN)

    pairs, passed = {}, {}
    for h in range(2):
        gather.begin(h)
    for h in range(2):
        pairs[h, 0] = gather.pair(h, gather.block(h))
    for off in (1, -1, 2):
        for h in range(2):
            gather.arrive(h, off)
            pairs[h, -off] = gather.pair(h, gather.block(h, -off))
    for first in (0, -1, 1, -2):
        for h in range(2):
            passed[h, first] = gather.relay(
                h, pairs[h, first],
                lambda second, h=h, first=first: gather.block(h, first, second),
                lambda ref, side: ref.at[side],
            )
        for h in range(2):
            project(h, first, 0)
            project(h, first, 1)
            project(h, first, -1)
    for first in (0, -1, 1, -2):
        for h in range(2):
            for copy in passed[h, first]:
                copy.wait_recv()
            project(h, first, 2)
    for h in range(2):
        part = pl.ds(h * (tokens // 2), tokens // 2)
        out_ref[part, :] = (residual_ref[part, :].astype(jnp.float32) + totals[h]).astype(jnp.bfloat16)


EXTRA = 128
SPREAD = ("y", "x")
SUM = ("x", "y")


def back_scratch(ff, features):
    quarter = ff // SIDE
    scratch = [pltpu.VMEM((N_SP, CAP, features), jnp.bfloat16) for _ in range(3)]
    for _ in range(2):
        scratch += [
            pltpu.VMEM((SIDE, features, 2 * quarter), jnp.bfloat16),
            pltpu.VMEM((PARTS, SIDE, 2, POS // 4 * CAP, features), jnp.bfloat16),
            pltpu.VMEM((PARTS, SIDE, SUB, 2 * quarter + EXTRA), jnp.bfloat16),
            pltpu.VMEM((PARTS, 3, SUB, 2 * quarter + EXTRA), jnp.bfloat16),
            pltpu.VMEM((PARTS, N_TP, 2, SUB // 2, quarter), jnp.bfloat16),
        ]
    return scratch


def spread_weights(place, copies, gain_ref, gate, up, scratch):
    gain = jnp.broadcast_to(gain_ref[...], (128, gain_ref.shape[1])).T[:, :1]
    quarter = gate.shape[1] // SIDE
    for matrix in (gate, up):
        matrix[...] = (matrix[...].astype(jnp.float32) * gain).astype(jnp.bfloat16)
    sent = []
    for h in range(2):
        target = scratch[3 + 5 * h]
        here = place.on(SPREAD[h])
        for n, matrix in enumerate((gate, up)):
            into = pl.ds(n * quarter, quarter)
            target[here, :, into] = matrix[:, pl.ds(pl.multiple_of(here * quarter, quarter), quarter)]
            for off in (2, 1, -1):
                columns = pl.ds(pl.multiple_of(place.on(SPREAD[h], off) * quarter, quarter), quarter)
                copy = copies(
                    matrix.at[:, columns], target.at[here, :, into], place.along(SPREAD[h], off)
                )
                copy.start()
                sent.append(copy)
    return sent


def peers_along_z(place):
    return [
        (2 * near + other, 2 * INVERSE[near] + other, place.at_z(off, bool(other)))
        for near, off in enumerate(OFFSETS)
        for other in range(2)
        if off != 0 or other
    ]


def back(
    place, copies, mid_ref, pick_ref, high_ref, low_ref, down_ref, out_ref, scratch,
):
    outgoing, results, returned = scratch[:3]
    weights, rows_in, products_of, others_of, hidden = zip(scratch[3:8], scratch[8:13])
    features = mid_ref.shape[1]
    quarter = hidden[0].shape[-1]
    z_peers = peers_along_z(place)

    def landing(at):
        part, i = at // POS, at % POS
        h, i = i // (POS // 2), i % (POS // 2)
        blocks = POS // 4
        return rows_in[h].at[part, place.on(SPREAD[h]), i // blocks, pl.ds(i % blocks * CAP, CAP)]

    for part in range(PARTS):
        rows = pl.ds(part * POS * CAP, POS * CAP)
        outgoing[pl.ds(part * POS, POS)] = (
            dot(pick_ref[rows, :], mid_ref[...], NN).astype(jnp.bfloat16).reshape(POS, CAP, features)
        )
    landing(HOME)[...] = outgoing[HOME]
    dispatch = {}
    for at, there, device in z_peers:
        dispatch[at] = copies(outgoing.at[at], landing(there), device)
        dispatch[at].start()
    lands = {there: dispatch[at] for at, there, _ in z_peers}
    back = {}
    state = [dict() for _ in range(PARTS)]
    gathers = [
        TorusGather(place, copies, [hidden[h].at[part] for h in range(2)]) for part in range(PARTS)
    ]

    def gather_rows(part):
        for at in range(part * POS, (part + 1) * POS):
            if at in lands:
                lands[at].wait_recv()
        for h in range(2):
            mine = rows_in[h].at[part, place.on(SPREAD[h])]
            sent = [copies(mine, mine, place.along(SPREAD[h], off)) for off in (1, -1)]
            for copy in sent:
                copy.start()
            state[part][h, "rows"] = sent

    def relay_rows(part, h):
        sent = []
        for side, off in ((0, 1), (1, -1)):
            state[part][h, "rows"][side].wait_recv()
            piece = rows_in[h].at[part, place.on(SPREAD[h], -off), side]
            sent.append(copies(piece, piece, place.along(SPREAD[h], off)))
            sent[-1].start()
        state[part][h, "relayed"] = sent

    def multiply(part, h):
        for copy in state[part][h, "relayed"]:
            copy.wait_recv()
        total, squares = 0.0, 0.0
        for p in range(SIDE):
            rows = rows_in[h][part, p].reshape(POS // 2 * CAP, features)
            total += dot(rows, weights[h][p], NN)
            squares += jnp.sum(jnp.square(rows.astype(jnp.float32)), axis=1, keepdims=True)
        extra = jnp.broadcast_to(squares, (POS // 2 * CAP, EXTRA))
        value = jnp.concatenate([total, extra], axis=1).astype(jnp.bfloat16)
        products_of[h][part] = value.reshape(SIDE, SUB, 2 * quarter + EXTRA)
        sent = []
        for n, off in enumerate((2, 1, -1)):
            sent.append(
                copies(
                    products_of[h].at[part, place.on(SUM[h], off)],
                    others_of[h].at[part, n],
                    place.along(SUM[h], off),
                )
            )
            sent[-1].start()
        state[part][h, "products"] = sent

    def activate(part, h):
        for copy in state[part][h, "products"]:
            copy.wait_recv()
        total = products_of[h][part, place.on(SUM[h])].astype(jnp.float32)
        for n in range(3):
            total += others_of[h][part, n].astype(jnp.float32)
        inv = lax.rsqrt(total[:, 2 * quarter : 2 * quarter + 1] * (1.0 / D) + EPS_NORM)
        gate = total[:, :quarter] * inv
        value = gate * sigmoid(gate) * (total[:, quarter : 2 * quarter] * inv)
        gather = gathers[part]
        hidden[h][part, gather.at(h)] = value.astype(jnp.bfloat16).reshape(2, SUB // 2, quarter)
        gather.begin(h)

    def second_axis(part, h):
        for off in (1, -1, 2):
            gathers[part].arrive(h, off)
        state[part][h, "pair"] = gathers[part].pair(h, gathers[part].row(h))

    def relay_hidden(part, h):
        gather = gathers[part]
        state[part][h, "passed"] = gather.relay(
            h, state[part][h, "pair"],
            lambda second: gather.row(h, second), lambda ref, side: ref.at[:, side],
        )

    def outputs(part):
        for h in range(2):
            for copy in state[part][h, "passed"]:
                copy.wait_recv()
            total = 0.0
            for p in range(SIDE):
                rows = hidden[h][part, pl.ds(p * SIDE, SIDE)].reshape(POS // 2 * CAP, quarter)
                total += dot(rows, down_ref[pl.ds(p * quarter, quarter), :], NN)
            first = part * POS + h * (POS // 2)
            results[pl.ds(first, POS // 2)] = total.astype(jnp.bfloat16).reshape(POS // 2, CAP, features)
        for at, there, device in z_peers:
            if part * POS <= at < (part + 1) * POS:
                back[at] = copies(results.at[at], returned.at[there], device)
                back[at].start()
        if part == HOME // POS:
            returned[HOME] = results[HOME]

    def both(action):
        def run(part):
            for h in range(2):
                action(part, h)
        return run

    stages = [
        gather_rows,
        both(relay_rows),
        both(multiply),
        both(activate),
        both(second_axis),
        both(relay_hidden),
        outputs,
    ]
    begins = (0.0, 7.0, 11.0, 13.0)
    plan = sorted(
        (begins[part] + 3.0 * n, part, n) for part in range(PARTS) for n in range(len(stages))
    )
    for _, part, n in plan:
        stages[n](part)

    came = {there: back[at] for at, there, _ in z_peers}
    total = mid_ref[...].astype(jnp.float32)
    for part in range(PARTS):
        for at in range(part * POS, (part + 1) * POS):
            if at in came:
                came[at].wait_recv()
        rows = returned[pl.ds(part * POS, POS)].reshape(POS * CAP, features)
        columns = pl.ds(part * POS * CAP, POS * CAP)
        total += dot(high_ref[columns, :], rows, TN) + dot(low_ref[columns, :], rows, TN)
    out_ref[...] = total.astype(jnp.bfloat16)


def kernel(
    r_ref, k_ref, v_ref, d_ref, a_ref, gate_logits_ref, group_gain_ref, residual_ref, norm_gain_ref,
    ids_ref, route_weight_ref, mixer_hbm, gate_hbm, up_hbm, down_hbm, out_ref, *scratch
):
    mixer, gate, up, down, loaded, send, recv = scratch[:7]
    reads, states, pick, high, low, midway, cores, maps, incoming = scratch[7:16]
    halves = scratch[16:18]
    place = Place()
    copies = Copies(send, recv)
    barrier = pltpu.get_barrier_semaphore()
    others = [peer[2] for peer in peers_along_z(place)]
    others += [place.along(axis, off) for axis in "xy" for off in (2, 1, -1)]
    for device in others:
        pl.semaphore_signal(barrier, inc=1, device_id=device, device_id_type=MESH)
    loads = [
        pltpu.make_async_copy(src, dst, loaded.at[n])
        for n, (src, dst) in enumerate(
            [(mixer_hbm, mixer), (gate_hbm, gate), (up_hbm, up), (down_hbm, down)]
        )
    ]
    for load in loads:
        load.start()
    for pair in range(r_ref.shape[1] // (2 * HEAD)):
        lanes = pl.ds(pair * 2 * HEAD, 2 * HEAD)
        mix_kernel(
            *[ref.at[:, lanes] for ref in (r_ref, k_ref, v_ref, d_ref, a_ref)],
            reads.at[:, pl.ds(pair * 4 * HEAD, 4 * HEAD)],
            states.at[lanes, :],
        )
    pl.semaphore_wait(barrier, len(others))

    spread = []

    def prepare_weights():
        for load in loads:
            load.wait()
        spread.extend(spread_weights(place, copies, norm_gain_ref, gate, up, scratch[18:]))

    meanwhile = [
        lambda: route(place, ids_ref, route_weight_ref, pick, high, low),
        prepare_weights,
    ]
    front(
        place, copies, meanwhile,
        reads, states, gate_logits_ref, group_gain_ref, mixer, residual_ref, midway,
        cores, maps, incoming, halves,
    )
    for copy in spread:
        copy.wait_recv()
    back(place, copies, midway, pick, high, low, down, out_ref, scratch[18:])
    copies.drain()


def local(
    receptance,
    key_vectors,
    value_vectors,
    decay_logits,
    rate_logits,
    gate_logits,
    group_gain,
    residual,
    mixer_out,
    norm_gain,
    expert_ids,
    route_weight,
    expert_gate,
    expert_up,
    expert_down,
):
    tokens, channels = residual.shape
    features = norm_gain.shape[0]
    ff = expert_gate.shape[2]
    slots = N_SP * CAP
    count = 2 + (NZ - 1) + 12 + 38 + 2 * (N_SP - 1) + PARTS * 28
    bf16 = jnp.bfloat16
    vmem = pl.BlockSpec(memory_space=pltpu.VMEM)
    hbm = pl.BlockSpec(memory_space=pl.ANY)
    weights = (mixer_out, expert_gate[0], expert_up[0], expert_down[0])
    return pl.pallas_call(
        kernel,
        in_specs=[vmem] * 11 + [hbm] * 4,
        out_specs=vmem,
        out_shape=jax.ShapeDtypeStruct((tokens, features), bf16),
        scratch_shapes=[pltpu.VMEM(w.shape, bf16) for w in weights]
        + [
            pltpu.SemaphoreType.DMA((len(weights),)),
            pltpu.SemaphoreType.DMA((count,)),
            pltpu.SemaphoreType.DMA((count,)),
            pltpu.VMEM((tokens, 2 * channels), jnp.float32),
            pltpu.VMEM((channels, 2 * HEAD), bf16),
            pltpu.VMEM((slots, tokens), bf16),
            pltpu.VMEM((slots, tokens), bf16),
            pltpu.VMEM((slots, tokens), bf16),
            pltpu.VMEM((tokens, features), bf16),
            pltpu.VMEM((2, channels, 2 * HEAD), bf16),
            pltpu.VMEM((NZ, channels // 2, 2 * HEAD), bf16),
            pltpu.VMEM((2, HEAD, channels // 2), jnp.float32),
            pltpu.VMEM((N_TP, 2, tokens // 4, channels), bf16),
            pltpu.VMEM((N_TP, 2, tokens // 4, channels), bf16),
        ]
        + back_scratch(ff, features),
        compiler_params=pltpu.CompilerParams(
            collective_id=0, has_side_effects=True, vmem_limit_bytes=60 * 1024 * 1024
        ),
        name="layer",
    )(
        receptance, key_vectors, value_vectors, decay_logits, rate_logits, gate_logits,
        group_gain.reshape(1, channels), residual, norm_gain.reshape(1, features),
        expert_ids.T, route_weight.T, *weights,
    )


def solution(mesh):
    placed = (
        P("sp", "tp"),
        P("sp", "tp"),
        P("sp", "tp"),
        P("sp", "tp"),
        P("sp", "tp"),
        P("sp", "tp"),
        P("tp"),
        P("sp", "tp"),
        P(None, "tp"),
        P("tp"),
        P("sp", None),
        P("sp", None),
        P("sp", "tp", None),
        P("sp", "tp", None),
        P("sp", None, "tp"),
    )
    return jax.shard_map(
        local, mesh=mesh, in_specs=placed, out_specs=P("sp", "tp"), check_vma=False
    )
```

```python
import jax
import jax.numpy as jnp
from jax import lax
from jax.experimental import pallas as pl
from jax.experimental.pallas import tpu as pltpu
from jax.sharding import PartitionSpec as P

D = 4096
HEAD = 64
CHUNK = 128
EXP_HALF = 0.6065306597126334

NZ = 16
N_SP = 2 * NZ
SIDE = 4
N_TP = SIDE * SIDE
CAP = 32
PARTS = 4
POS = N_SP // PARTS
SUB = POS * CAP // 8

EPS_GROUP = 0.00064
EPS_NORM = 1e-06
MESH = pl.DeviceIdType.MESH

OFFSETS = [NZ // 2]
for _far in range(NZ // 2 - 1, 0, -1):
    OFFSETS += [_far, -_far]
OFFSETS += [0]
HOME = N_SP - 2
INVERSE = [OFFSETS.index(-o if o != NZ // 2 else o) for o in OFFSETS]


def split(x):
    hi = x.astype(jnp.bfloat16)
    lo = (x - hi.astype(jnp.float32)).astype(jnp.bfloat16)
    return hi, lo


def dot(a, b, dims):
    return lax.dot_general(a, b, (dims, ((), ())), preferred_element_type=jnp.float32)


NN = ((1,), (0,))
NT = ((1,), (1,))
TN = ((0,), (0,))


def dot3(a, b, dims=NN):
    return dot(a[0], b[0], dims) + (dot(a[0], b[1], dims) + dot(a[1], b[0], dims))


def dot2(a, b, dims=NN):
    return dot(a[0], b, dims) + dot(a[1], b, dims)


def side(*parts):
    return jnp.concatenate(parts, axis=1)


def stack(*parts):
    return jnp.concatenate(parts, axis=0)


def packed(a, b):
    width = b[0].shape[1]
    both = side(*b)
    total = dot(a, stack(both, both), NN)
    return total[:, :width] + total[:, width:]


def sigmoid(x):
    return 1.0 / (1.0 + jnp.exp(-x))


def mix(r_ref, k_ref, v_ref, d_ref, a_ref, out_ref, state_ref):
    tokens = r_ref.shape[0]
    chunks = tokens // CHUNK
    row = lax.broadcasted_iota(jnp.int32, (CHUNK, CHUNK), 0)
    col = lax.broadcasted_iota(jnp.int32, (CHUNK, CHUNK), 1)
    strict = col < row
    causal = col <= row
    eye = jnp.where(col == row, 1.0, 0.0)
    ones_lower = jnp.where(causal, 1.0, 0.0).astype(jnp.bfloat16)
    low = lax.broadcasted_iota(jnp.int32, (CHUNK, 2 * HEAD), 1) < HEAD

    work = []
    pairs = r_ref.shape[1] // (2 * HEAD)
    for chunk, pair in [(c, p) for c in range(chunks) for p in range(pairs)]:
        rows = pl.ds(chunk * CHUNK, CHUNK)
        wide = pl.ds(pair * 2 * HEAD, 2 * HEAD)
        recept = r_ref[rows, wide].astype(jnp.float32)
        keyvec = k_ref[rows, wide].astype(jnp.float32)
        logdec = -EXP_HALF * sigmoid(d_ref[rows, wide].astype(jnp.float32))
        first, second = split(logdec)
        third = (logdec - first.astype(jnp.float32) - second.astype(jnp.float32)).astype(jnp.bfloat16)
        cum_two = dot(ones_lower, side(first, second), NN)
        cum_in = cum_two[:, : 2 * HEAD] + (cum_two[:, 2 * HEAD :] + dot(ones_lower, third, NN))
        cum_end = cum_in[CHUNK - 1 :, :]
        squares = keyvec * keyvec
        norms = jnp.where(
            low,
            jnp.sum(squares[:, :HEAD], axis=1, keepdims=True),
            jnp.sum(squares[:, HEAD:], axis=1, keepdims=True),
        )
        unit_key = keyvec * lax.rsqrt(1.0 + norms)
        correction = unit_key * sigmoid(a_ref[rows, wide].astype(jnp.float32))
        growth = jnp.exp(-cum_in)
        tail = jnp.exp(cum_end - cum_in)
        r_scaled = recept * jnp.exp(cum_in)
        u_scaled = unit_key * jnp.exp(cum_in - logdec)
        queries = split(jnp.concatenate([u_scaled, r_scaled], axis=0))
        sources = split(jnp.concatenate([keyvec * growth, correction * growth], axis=0))
        tails = split(jnp.concatenate([keyvec * tail, -(correction * tail)], axis=0))
        keep = jnp.broadcast_to(jnp.exp(cum_end), (2 * HEAD, 2 * HEAD)).T
        values = v_ref[rows, wide]
        for head in range(2):
            lanes = slice(head * HEAD, (head + 1) * HEAD)
            query = side(*[q[:, lanes] for q in queries])
            near, rest = [s[:, lanes] for s in sources]
            scores = dot(side(query, query), side(near, near, rest, rest), NT)
            work.append(
                dict(
                    head=pair * 2 + head,
                    chunk=chunk,
                    query=query,
                    tail=tuple(t[:, lanes] for t in tails),
                    keep=keep[lanes, :],
                    value=jnp.concatenate(
                        [values[:, lanes], jnp.zeros((CHUNK, HEAD), jnp.bfloat16)], axis=1
                    ),
                    key_both=split(
                        jnp.concatenate(
                            [
                                jnp.where(strict, scores[:CHUNK, :CHUNK], 0.0),
                                jnp.where(causal, scores[CHUNK:, :CHUNK], 0.0),
                            ],
                            axis=0,
                        )
                    ),
                    pull=jnp.where(strict, scores[:CHUNK, CHUNK:], 0.0),
                    corr_read=split(jnp.where(causal, scores[CHUNK:, CHUNK:], 0.0)),
                )
            )
    for item in work:
        item["inverse"] = eye - jnp.where(row // 2 == col // 2, item["pull"], 0.0)
        item["from_values"] = dot(side(*item["key_both"]), stack(item["value"], item["value"]), NN)
    size = 2
    while size < CHUNK:
        joined = (row // (2 * size) == col // (2 * size)) & (row // size != col // size)
        halves = []
        for item in work:
            inverse = split(item["inverse"])
            between = split(jnp.where(joined, item["pull"], 0.0))
            halves.append((inverse, packed(side(*between), inverse)))
        for item, (inverse, half) in zip(work, halves):
            item["inverse"] = item["inverse"] - packed(side(*inverse), split(half))
        size *= 2
    key_row = lax.broadcasted_iota(jnp.int32, (HEAD, 2 * HEAD), 0)
    lane = lax.broadcasted_iota(jnp.int32, (HEAD, 2 * HEAD), 1)
    start = jnp.where(lane == key_row + HEAD, 1.0, 0.0)
    states = [start] * (2 * pairs)
    for item in work:
        head = item["head"]
        state = states[head]
        from_start = packed(item["query"], split(state)) + item["from_values"]
        pulled = packed(side(*split(item["inverse"])), split(from_start[:CHUNK]))
        pulled_parts = split(pulled)
        out_ref[pl.ds(item["chunk"] * CHUNK, CHUNK), pl.ds(head * 2 * HEAD, 2 * HEAD)] = (
            from_start[CHUNK:] - packed(side(*item["corr_read"]), pulled_parts)
        )
        key_tail = tuple(t[:CHUNK] for t in item["tail"])
        corr_tail = tuple(t[CHUNK:] for t in item["tail"])
        states[head] = (
            item["keep"] * state
            + dot2(key_tail, item["value"], TN)
            + dot3(corr_tail, pulled_parts, TN)
        )
    for head in range(2 * pairs):
        state_ref[pl.ds(head * HEAD, HEAD), :] = states[head].astype(jnp.bfloat16)


def route(place, ids_ref, weight_ref, pick_ref, high_ref, low_ref):
    tokens = ids_ref.shape[1]
    slots = N_SP * CAP
    expert = lax.broadcasted_iota(jnp.int32, (128, tokens), 0)
    named = [ids_ref[k : k + 1, :] == expert for k in range(2)]
    onehot = jnp.where(named[0] | named[1], 1.0, 0.0).astype(jnp.bfloat16)
    row = lax.broadcasted_iota(jnp.int32, (tokens, tokens), 0)
    col = lax.broadcasted_iota(jnp.int32, (tokens, tokens), 1)
    before = jnp.where(row < col, 1.0, 0.0).astype(jnp.bfloat16)
    earlier = dot(onehot, before, NN).astype(jnp.bfloat16)
    weight = jnp.where(named[0], weight_ref[0:1, :], 0.0) + jnp.where(named[1], weight_ref[1:2, :], 0.0)
    high, low = split(weight)
    slot = lax.broadcasted_iota(jnp.int32, (slots, 128), 0)
    source = lax.broadcasted_iota(jnp.int32, (slots, 128), 1)
    near = slot // (2 * CAP)
    step = NZ // 2 - (near + 1) // 2
    off = jnp.where(near % 2 == 1, step, NZ - step)
    chip = (place.z + off) % NZ
    core = (place.core + slot // CAP) % 2
    spread = jnp.where(source == chip * 2 + core, 1.0, 0.0).astype(jnp.bfloat16)
    rank = (lax.broadcasted_iota(jnp.int32, (slots, tokens), 0) % CAP).astype(jnp.float32)
    taken = jnp.where(dot(spread, earlier, NN) == rank, dot(spread, onehot, NN), 0.0)
    pick_ref[...] = taken.astype(jnp.bfloat16)
    high_ref[...] = (taken * dot(spread, high, NN)).astype(jnp.bfloat16)
    low_ref[...] = (taken * dot(spread, low, NN)).astype(jnp.bfloat16)


class Place:
    def __init__(self):
        self.sp = lax.axis_index("sp")
        self.tp = lax.axis_index("tp")
        self.z, self.core = self.sp // 2, self.sp % 2
        self.y, self.x = self.tp // SIDE, self.tp % SIDE

    def chip(self, off, other=False):
        core = (self.core + 1) % 2 if other else self.core
        return ((self.z + off + NZ) % NZ) * 2 + core

    def at_z(self, off, other=False):
        return {"sp": self.chip(off, other), "tp": self.tp}

    def along(self, axis, off):
        if axis == "x":
            return {"sp": self.sp, "tp": self.y * SIDE + (self.x + off + SIDE) % SIDE}
        return {"sp": self.sp, "tp": ((self.y + off + SIDE) % SIDE) * SIDE + self.x}

    def on(self, axis, off=0):
        return ((self.x if axis == "x" else self.y) + off + SIDE) % SIDE


class Copies:
    def __init__(self, send, recv):
        self.send, self.recv = send, recv
        self.made = []

    def __call__(self, src, dst, device):
        index = len(self.made)
        copy = pltpu.make_async_remote_copy(
            src_ref=src,
            dst_ref=dst,
            send_sem=self.send.at[index],
            recv_sem=self.recv.at[index],
            device_id=device,
            device_id_type=MESH,
        )
        self.made.append(copy)
        return copy

    def drain(self):
        for copy in self.made:
            copy.wait_send()


ORDER = (("x", "y"), ("y", "x"))


class TorusGather:
    def __init__(self, place, copies, blocks):
        self.place, self.copies, self.blocks = place, copies, blocks
        self.state = [dict() for _ in blocks]

    def at(self, h, first=0, second=0):
        one, two = ORDER[h]
        return self.place.on(two, second) * SIDE + self.place.on(one, first)

    def block(self, h, first=0, second=0):
        return self.blocks[h].at[self.at(h, first, second)]

    def row(self, h, second=0):
        start = self.place.on(ORDER[h][1], second) * SIDE
        return self.blocks[h].at[pl.ds(start, SIDE)]

    def begin(self, h):
        mine = self.block(h)
        sent = {off: self.copies(mine, mine, self.place.along(ORDER[h][0], off)) for off in (2, 1, -1)}
        for copy in sent.values():
            copy.start()
        self.state[h]["first"] = sent

    def arrive(self, h, off):
        self.state[h]["first"][off].wait_recv()

    def pair(self, h, ref):
        sent = [self.copies(ref, ref, self.place.along(ORDER[h][1], off)) for off in (1, -1)]
        for copy in sent:
            copy.start()
        return sent

    def relay(self, h, sent, ref_of, half):
        passed = []
        for side, (copy, off) in enumerate(zip(sent, (1, -1))):
            copy.wait_recv()
            piece = half(ref_of(-off), side)
            passed.append(self.copies(piece, piece, self.place.along(ORDER[h][1], off)))
            passed[-1].start()
        return passed


def front(
    place, copies, meanwhile,
    reads_ref, states_ref, gate_ref, gain_ref, weight_ref, residual_ref, out_ref,
    cores, maps, incoming_ref, halves,
):
    partner = place.at_z(0, True)
    tokens = out_ref.shape[0]
    heads = states_ref.shape[0] // HEAD
    mine = heads // 2
    cores[place.core] = states_ref[...]
    swap = copies(states_ref, cores.at[place.core], partner)
    swap.start()
    swap.wait_recv()
    for head in range(mine):
        rows = pl.ds(pl.multiple_of((place.core * mine + head) * HEAD, HEAD), HEAD)
        later = cores[1, rows, :]
        added = dot(later[:, HEAD:], cores[0, rows, :], NN)
        state = later[:, :HEAD].astype(jnp.float32) + added[:, :HEAD]
        maps[place.z, pl.ds(head * HEAD, HEAD), :] = jnp.concatenate(
            [state, added[:, HEAD:]], axis=1
        ).astype(jnp.bfloat16)

    came = {}
    last = {1: NZ // 2, -1: NZ // 2 - 1}

    def pass_on(direction, d):
        ref = maps.at[(place.z - direction * d + NZ) % NZ]
        for far in (2, 1):
            if d + far <= last[direction]:
                came[direction, d + far] = copies(ref, ref, place.at_z(direction * far))
                came[direction, d + far].start()

    def step_of(d, head):
        both = maps[(place.z - d + NZ) % NZ, pl.ds(head * HEAD, HEAD), :]
        return jnp.where(place.z >= d, both, unit)

    lane = lax.broadcasted_iota(jnp.int32, (HEAD, 2 * HEAD), 1)
    row = lax.broadcasted_iota(jnp.int32, (HEAD, 2 * HEAD), 0)
    identity = jnp.where(lane == row + HEAD, 1.0, 0.0)
    unit = identity.astype(jnp.bfloat16)
    window = [identity] * mine
    far = [jnp.zeros((HEAD, HEAD), jnp.float32)] * mine

    def take(direction, d):
        for head in range(mine):
            if direction > 0:
                both = step_of(d, head)
                hi, lo = split(window[head][:, HEAD:])
                added = dot(hi, both, NN) + dot(lo, both, NN)
                window[head] = side(window[head][:, :HEAD] + added[:, :HEAD], added[:, HEAD:])
            else:
                both = step_of(NZ - d, head)
                hi, lo = split(far[head])
                step_map = both[:, HEAD:]
                far[head] = (
                    both[:, :HEAD].astype(jnp.float32) + dot(step_map, hi, NN) + dot(step_map, lo, NN)
                )

    for d in range(0, NZ // 2, 2):
        for direction in (1, -1):
            if d:
                came[direction, d].wait_recv()
            pass_on(direction, d)
        if d:
            for direction in (1, -1):
                came[direction, d - 1].wait_recv()
                take(direction, d - 1)
                take(direction, d)
        if d // 2 < len(meanwhile):
            meanwhile[d // 2]()
    for direction in (1, -1):
        for d in (NZ // 2 - 1, NZ // 2):
            if d <= last[direction]:
                came[direction, d].wait_recv()
                take(direction, d)
    incoming = [
        window[head][:, :HEAD] + dot3(split(window[head][:, HEAD:]), split(far[head]))
        for head in range(mine)
    ]
    incoming_ref[place.core] = side(*incoming)
    swap = copies(incoming_ref.at[place.core], incoming_ref.at[place.core], partner)
    swap.start()
    second = (jnp.zeros((HEAD, HEAD), jnp.int32) + place.core) == 1
    swap.wait_recv()
    scaled = []
    for head in range(heads):
        before = incoming_ref[head // mine, :, (head % mine) * HEAD : (head % mine + 1) * HEAD]
        both = cores[0, pl.ds(head * HEAD, HEAD), :]
        hi, lo = split(before)
        step_map = both[:, HEAD:]
        after = both[:, :HEAD].astype(jnp.float32) + dot(step_map, hi, NN) + dot(step_map, lo, NN)
        state = jnp.where(second, after, before)
        both = reads_ref[:, pl.ds(head * 2 * HEAD, 2 * HEAD)]
        state_read = both[:, :HEAD] + dot3(split(both[:, HEAD:]), split(state))
        centred = state_read - jnp.mean(state_read, axis=1, keepdims=True)
        variance = jnp.mean(centred * centred, axis=1, keepdims=True)
        scaled.append(centred * lax.rsqrt(variance + EPS_GROUP))
    gated = (
        jnp.concatenate(scaled, axis=1)
        * gain_ref[...]
        * sigmoid(gate_ref[...].astype(jnp.float32))
    ).astype(jnp.bfloat16)
    gather = TorusGather(place, copies, halves)
    quarter = tokens // 4
    for h in range(2):
        for q in range(2):
            at = (2 * h + q) * quarter
            halves[h][gather.at(h), q] = gated[at : at + quarter]
    width = gated.shape[1]
    totals = [jnp.zeros((tokens // 2, out_ref.shape[1]), jnp.float32) for _ in range(2)]

    def project(h, first, second):
        x, y = (first, second) if h == 0 else (second, first)
        t = place.on("y", y) * SIDE + place.on("x", x)
        rows = pl.ds(pl.multiple_of(t * width, width), width)
        block = halves[h][gather.at(h, first, second)].reshape(tokens // 2, width)
        totals[h] += dot(block, weight_ref[rows, :], NN)

    pairs, passed = {}, {}
    for h in range(2):
        gather.begin(h)
    for h in range(2):
        pairs[h, 0] = gather.pair(h, gather.block(h))
    for off in (1, -1, 2):
        for h in range(2):
            gather.arrive(h, off)
            pairs[h, -off] = gather.pair(h, gather.block(h, -off))
    for first in (0, -1, 1, -2):
        for h in range(2):
            passed[h, first] = gather.relay(
                h, pairs[h, first],
                lambda second, h=h, first=first: gather.block(h, first, second),
                lambda ref, side: ref.at[side],
            )
        for h in range(2):
            project(h, first, 0)
            project(h, first, 1)
            project(h, first, -1)
    for first in (0, -1, 1, -2):
        for h in range(2):
            for copy in passed[h, first]:
                copy.wait_recv()
            project(h, first, 2)
    for h in range(2):
        part = pl.ds(h * (tokens // 2), tokens // 2)
        out_ref[part, :] = (residual_ref[part, :].astype(jnp.float32) + totals[h]).astype(jnp.bfloat16)


EXTRA = 128
SPREAD = ("y", "x")
SUM = ("x", "y")


def back_scratch(ff, features):
    quarter = ff // SIDE
    scratch = [pltpu.VMEM((N_SP, CAP, features), jnp.bfloat16) for _ in range(3)]
    for _ in range(2):
        scratch += [
            pltpu.VMEM((SIDE, features, 2 * quarter), jnp.bfloat16),
            pltpu.VMEM((PARTS, SIDE, 2, POS // 4 * CAP, features), jnp.bfloat16),
            pltpu.VMEM((PARTS, SIDE, SUB, 2 * quarter + EXTRA), jnp.bfloat16),
            pltpu.VMEM((PARTS, 3, SUB, 2 * quarter + EXTRA), jnp.bfloat16),
            pltpu.VMEM((PARTS, N_TP, 2, SUB // 2, quarter), jnp.bfloat16),
        ]
    return scratch


def spread_weights(place, copies, gain_ref, gate, up, scratch):
    gain = jnp.broadcast_to(gain_ref[...], (128, gain_ref.shape[1])).T[:, :1]
    quarter = gate.shape[1] // SIDE
    for matrix in (gate, up):
        matrix[...] = (matrix[...].astype(jnp.float32) * gain).astype(jnp.bfloat16)
    sent = []
    for h in range(2):
        target = scratch[3 + 5 * h]
        here = place.on(SPREAD[h])
        for n, matrix in enumerate((gate, up)):
            into = pl.ds(n * quarter, quarter)
            target[here, :, into] = matrix[:, pl.ds(pl.multiple_of(here * quarter, quarter), quarter)]
            for off in (2, 1, -1):
                columns = pl.ds(pl.multiple_of(place.on(SPREAD[h], off) * quarter, quarter), quarter)
                copy = copies(
                    matrix.at[:, columns], target.at[here, :, into], place.along(SPREAD[h], off)
                )
                copy.start()
                sent.append(copy)
    return sent


def peers_along_z(place):
    return [
        (2 * near + other, 2 * INVERSE[near] + other, place.at_z(off, bool(other)))
        for near, off in enumerate(OFFSETS)
        for other in range(2)
        if off != 0 or other
    ]


def back(
    place, copies, mid_ref, pick_ref, high_ref, low_ref, down_ref, out_ref, scratch,
):
    outgoing, results, returned = scratch[:3]
    weights, rows_in, products_of, others_of, hidden = zip(scratch[3:8], scratch[8:13])
    features = mid_ref.shape[1]
    quarter = hidden[0].shape[-1]
    z_peers = peers_along_z(place)

    def landing(at):
        part, i = at // POS, at % POS
        h, i = i // (POS // 2), i % (POS // 2)
        blocks = POS // 4
        return rows_in[h].at[part, place.on(SPREAD[h]), i // blocks, pl.ds(i % blocks * CAP, CAP)]

    dispatch = {}
    for part in range(PARTS):
        rows = pl.ds(part * POS * CAP, POS * CAP)
        outgoing[pl.ds(part * POS, POS)] = (
            dot(pick_ref[rows, :], mid_ref[...], NN).astype(jnp.bfloat16).reshape(POS, CAP, features)
        )
        for at, there, device in z_peers:
            if part * POS <= at < (part + 1) * POS:
                dispatch[at] = copies(outgoing.at[at], landing(there), device)
                dispatch[at].start()
    landing(HOME)[...] = outgoing[HOME]
    lands = {there: dispatch[at] for at, there, _ in z_peers}
    back = {}
    state = [dict() for _ in range(PARTS)]
    gathers = [
        TorusGather(place, copies, [hidden[h].at[part] for h in range(2)]) for part in range(PARTS)
    ]

    def gather_rows(part):
        for at in range(part * POS, (part + 1) * POS):
            if at in lands:
                lands[at].wait_recv()
        for h in range(2):
            mine = rows_in[h].at[part, place.on(SPREAD[h])]
            sent = [copies(mine, mine, place.along(SPREAD[h], off)) for off in (1, -1)]
            for copy in sent:
                copy.start()
            state[part][h, "rows"] = sent

    def relay_rows(part, h):
        sent = []
        for side, off in ((0, 1), (1, -1)):
            state[part][h, "rows"][side].wait_recv()
            piece = rows_in[h].at[part, place.on(SPREAD[h], -off), side]
            sent.append(copies(piece, piece, place.along(SPREAD[h], off)))
            sent[-1].start()
        state[part][h, "relayed"] = sent

    def multiply(part, h):
        for copy in state[part][h, "relayed"]:
            copy.wait_recv()
        total, squares = 0.0, 0.0
        for p in range(SIDE):
            rows = rows_in[h][part, p].reshape(POS // 2 * CAP, features)
            total += dot(rows, weights[h][p], NN)
            squares += jnp.sum(jnp.square(rows.astype(jnp.float32)), axis=1, keepdims=True)
        extra = jnp.broadcast_to(squares, (POS // 2 * CAP, EXTRA))
        value = jnp.concatenate([total, extra], axis=1).astype(jnp.bfloat16)
        products_of[h][part] = value.reshape(SIDE, SUB, 2 * quarter + EXTRA)
        sent = []
        for n, off in enumerate((2, 1, -1)):
            sent.append(
                copies(
                    products_of[h].at[part, place.on(SUM[h], off)],
                    others_of[h].at[part, n],
                    place.along(SUM[h], off),
                )
            )
            sent[-1].start()
        state[part][h, "products"] = sent

    def activate(part, h):
        for copy in state[part][h, "products"]:
            copy.wait_recv()
        total = products_of[h][part, place.on(SUM[h])].astype(jnp.float32)
        for n in range(3):
            total += others_of[h][part, n].astype(jnp.float32)
        inv = lax.rsqrt(total[:, 2 * quarter : 2 * quarter + 1] * (1.0 / D) + EPS_NORM)
        gate = total[:, :quarter] * inv
        value = gate * sigmoid(gate) * (total[:, quarter : 2 * quarter] * inv)
        gather = gathers[part]
        hidden[h][part, gather.at(h)] = value.astype(jnp.bfloat16).reshape(2, SUB // 2, quarter)
        gather.begin(h)

    def second_axis(part, h):
        for off in (1, -1, 2):
            gathers[part].arrive(h, off)
        state[part][h, "pair"] = gathers[part].pair(h, gathers[part].row(h))

    def relay_hidden(part, h):
        gather = gathers[part]
        state[part][h, "passed"] = gather.relay(
            h, state[part][h, "pair"],
            lambda second: gather.row(h, second), lambda ref, side: ref.at[:, side],
        )

    def outputs(part):
        for h in range(2):
            for copy in state[part][h, "passed"]:
                copy.wait_recv()
            total = 0.0
            for p in range(SIDE):
                rows = hidden[h][part, pl.ds(p * SIDE, SIDE)].reshape(POS // 2 * CAP, quarter)
                total += dot(rows, down_ref[pl.ds(p * quarter, quarter), :], NN)
            first = part * POS + h * (POS // 2)
            results[pl.ds(first, POS // 2)] = total.astype(jnp.bfloat16).reshape(POS // 2, CAP, features)
        for at, there, device in z_peers:
            if part * POS <= at < (part + 1) * POS:
                back[at] = copies(results.at[at], returned.at[there], device)
                back[at].start()
        if part == HOME // POS:
            returned[HOME] = results[HOME]

    def both(action):
        def run(part):
            for h in range(2):
                action(part, h)
        return run

    stages = [
        gather_rows,
        both(relay_rows),
        both(multiply),
        both(activate),
        both(second_axis),
        both(relay_hidden),
        outputs,
    ]
    begins = (0.0, 7.0, 11.0, 13.0)
    plan = sorted(
        (begins[part] + 3.0 * n, part, n) for part in range(PARTS) for n in range(len(stages))
    )
    for _, part, n in plan:
        stages[n](part)

    came = {there: back[at] for at, there, _ in z_peers}
    total = mid_ref[...].astype(jnp.float32)
    for part in range(PARTS):
        for at in range(part * POS, (part + 1) * POS):
            if at in came:
                came[at].wait_recv()
        rows = returned[pl.ds(part * POS, POS)].reshape(POS * CAP, features)
        columns = pl.ds(part * POS * CAP, POS * CAP)
        total += dot(high_ref[columns, :], rows, TN) + dot(low_ref[columns, :], rows, TN)
    out_ref[...] = total


def kernel(
    r_ref, k_ref, v_ref, d_ref, a_ref, gate_logits_ref, group_gain_ref, residual_ref, norm_gain_ref,
    ids_ref, route_weight_ref, mixer_hbm, gate_hbm, up_hbm, down_hbm, out_ref, *scratch
):
    mixer, gate, up, down, loaded, send, recv = scratch[:7]
    reads, states, pick, high, low, midway, cores, maps, incoming = scratch[7:16]
    halves = scratch[16:18]
    place = Place()
    copies = Copies(send, recv)
    barrier = pltpu.get_barrier_semaphore()
    others = [peer[2] for peer in peers_along_z(place)]
    others += [place.along(axis, off) for axis in "xy" for off in (2, 1, -1)]
    for device in others:
        pl.semaphore_signal(barrier, inc=1, device_id=device, device_id_type=MESH)
    loads = [
        pltpu.make_async_copy(src, dst, loaded.at[n])
        for n, (src, dst) in enumerate(
            [(mixer_hbm, mixer), (gate_hbm, gate), (up_hbm, up), (down_hbm, down)]
        )
    ]
    for load in loads:
        load.start()
    mix(r_ref, k_ref, v_ref, d_ref, a_ref, reads, states)
    pl.semaphore_wait(barrier, len(others))

    spread = []

    def prepare_weights():
        for load in loads:
            load.wait()
        spread.extend(spread_weights(place, copies, norm_gain_ref, gate, up, scratch[18:]))

    meanwhile = [
        lambda: route(place, ids_ref, route_weight_ref, pick, high, low),
        prepare_weights,
    ]
    front(
        place, copies, meanwhile,
        reads, states, gate_logits_ref, group_gain_ref, mixer, residual_ref, midway,
        cores, maps, incoming, halves,
    )
    for copy in spread:
        copy.wait_recv()
    back(place, copies, midway, pick, high, low, down, out_ref, scratch[18:])
    copies.drain()


def local(
    receptance,
    key_vectors,
    value_vectors,
    decay_logits,
    rate_logits,
    gate_logits,
    group_gain,
    residual,
    mixer_out,
    norm_gain,
    expert_ids,
    route_weight,
    expert_gate,
    expert_up,
    expert_down,
):
    tokens, channels = residual.shape
    features = norm_gain.shape[0]
    ff = expert_gate.shape[2]
    slots = N_SP * CAP
    count = 2 + (NZ - 1) + 12 + 38 + 2 * (N_SP - 1) + PARTS * 28
    bf16 = jnp.bfloat16
    vmem = pl.BlockSpec(memory_space=pltpu.VMEM)
    hbm = pl.BlockSpec(memory_space=pl.ANY)
    weights = (mixer_out, expert_gate[0], expert_up[0], expert_down[0])
    return pl.pallas_call(
        kernel,
        in_specs=[vmem] * 11 + [hbm] * 4,
        out_specs=vmem,
        out_shape=jax.ShapeDtypeStruct((tokens, features), jnp.float32),
        scratch_shapes=[pltpu.VMEM(w.shape, bf16) for w in weights]
        + [
            pltpu.SemaphoreType.DMA((len(weights),)),
            pltpu.SemaphoreType.DMA((count,)),
            pltpu.SemaphoreType.DMA((count,)),
            pltpu.VMEM((tokens, 2 * channels), jnp.float32),
            pltpu.VMEM((channels, 2 * HEAD), bf16),
            pltpu.VMEM((slots, tokens), bf16),
            pltpu.VMEM((slots, tokens), bf16),
            pltpu.VMEM((slots, tokens), bf16),
            pltpu.VMEM((tokens, features), bf16),
            pltpu.VMEM((2, channels, 2 * HEAD), bf16),
            pltpu.VMEM((NZ, channels // 2, 2 * HEAD), bf16),
            pltpu.VMEM((2, HEAD, channels // 2), jnp.float32),
            pltpu.VMEM((N_TP, 2, tokens // 4, channels), bf16),
            pltpu.VMEM((N_TP, 2, tokens // 4, channels), bf16),
        ]
        + back_scratch(ff, features),
        compiler_params=pltpu.CompilerParams(
            collective_id=0, has_side_effects=True, vmem_limit_bytes=60 * 1024 * 1024
        ),
        name="layer",
    )(
        receptance, key_vectors, value_vectors, decay_logits, rate_logits, gate_logits,
        group_gain.reshape(1, channels), residual, norm_gain.reshape(1, features),
        expert_ids.T, route_weight.T, *weights,
    ).astype(bf16)


def solution(mesh):
    placed = (
        P("sp", "tp"),
        P("sp", "tp"),
        P("sp", "tp"),
        P("sp", "tp"),
        P("sp", "tp"),
        P("sp", "tp"),
        P("tp"),
        P("sp", "tp"),
        P(None, "tp"),
        P("tp"),
        P("sp", None),
        P("sp", None),
        P("sp", "tp", None),
        P("sp", "tp", None),
        P("sp", None, "tp"),
    )
    return jax.shard_map(
        local, mesh=mesh, in_specs=placed, out_specs=P("sp", "tp"), check_vma=False
    )
```

```python
import jax
import jax.numpy as jnp
from jax import lax
from jax.experimental import pallas as pl
from jax.experimental.pallas import tpu as pltpu
from jax.sharding import PartitionSpec as P

D = 4096
HEAD = 64
CHUNK = 128
EXP_HALF = 0.6065306597126334

NZ = 16
N_SP = 2 * NZ
SIDE = 4
N_TP = SIDE * SIDE
CAP = 32
PARTS = 4
POS = N_SP // PARTS
SUB = POS * CAP // 8

EPS_GROUP = 0.00064
EPS_NORM = 1e-06
MESH = pl.DeviceIdType.MESH

OFFSETS = [NZ // 2]
for _far in range(NZ // 2 - 1, 0, -1):
    OFFSETS += [_far, -_far]
OFFSETS += [0]
HOME = N_SP - 2
INVERSE = [OFFSETS.index(-o if o != NZ // 2 else o) for o in OFFSETS]


def split(x):
    hi = x.astype(jnp.bfloat16)
    lo = (x - hi.astype(jnp.float32)).astype(jnp.bfloat16)
    return hi, lo


def dot(a, b, dims):
    return lax.dot_general(a, b, (dims, ((), ())), preferred_element_type=jnp.float32)


NN = ((1,), (0,))
NT = ((1,), (1,))
TN = ((0,), (0,))


def dot3(a, b, dims=NN):
    return dot(a[0], b[0], dims) + (dot(a[0], b[1], dims) + dot(a[1], b[0], dims))


def dot2(a, b, dims=NN):
    return dot(a[0], b, dims) + dot(a[1], b, dims)


def side(*parts):
    return jnp.concatenate(parts, axis=1)


def stack(*parts):
    return jnp.concatenate(parts, axis=0)


def packed(a, b):
    width = b[0].shape[1]
    both = side(*b)
    total = dot(a, stack(both, both), NN)
    return total[:, :width] + total[:, width:]


def sigmoid(x):
    return 1.0 / (1.0 + jnp.exp(-x))


def mix(r_ref, k_ref, v_ref, d_ref, a_ref, out_ref, state_ref):
    tokens = r_ref.shape[0]
    chunks = tokens // CHUNK
    row = lax.broadcasted_iota(jnp.int32, (CHUNK, CHUNK), 0)
    col = lax.broadcasted_iota(jnp.int32, (CHUNK, CHUNK), 1)
    strict = col < row
    causal = col <= row
    eye = jnp.where(col == row, 1.0, 0.0)
    ones_lower = jnp.where(causal, 1.0, 0.0).astype(jnp.bfloat16)
    low = lax.broadcasted_iota(jnp.int32, (CHUNK, 2 * HEAD), 1) < HEAD

    work = []
    pairs = r_ref.shape[1] // (2 * HEAD)
    for chunk, pair in [(c, p) for c in range(chunks) for p in range(pairs)]:
        rows = pl.ds(chunk * CHUNK, CHUNK)
        wide = pl.ds(pair * 2 * HEAD, 2 * HEAD)
        recept = r_ref[rows, wide].astype(jnp.float32)
        keyvec = k_ref[rows, wide].astype(jnp.float32)
        logdec = -EXP_HALF * sigmoid(d_ref[rows, wide].astype(jnp.float32))
        first, second = split(logdec)
        third = (logdec - first.astype(jnp.float32) - second.astype(jnp.float32)).astype(jnp.bfloat16)
        cum_two = dot(ones_lower, side(first, second), NN)
        cum_in = cum_two[:, : 2 * HEAD] + (cum_two[:, 2 * HEAD :] + dot(ones_lower, third, NN))
        cum_end = cum_in[CHUNK - 1 :, :]
        squares = keyvec * keyvec
        norms = jnp.where(
            low,
            jnp.sum(squares[:, :HEAD], axis=1, keepdims=True),
            jnp.sum(squares[:, HEAD:], axis=1, keepdims=True),
        )
        unit_key = keyvec * lax.rsqrt(1.0 + norms)
        correction = unit_key * sigmoid(a_ref[rows, wide].astype(jnp.float32))
        growth = jnp.exp(-cum_in)
        tail = jnp.exp(cum_end - cum_in)
        r_scaled = recept * jnp.exp(cum_in)
        u_scaled = unit_key * jnp.exp(cum_in - logdec)
        queries = split(jnp.concatenate([u_scaled, r_scaled], axis=0))
        sources = split(jnp.concatenate([keyvec * growth, correction * growth], axis=0))
        tails = split(jnp.concatenate([keyvec * tail, -(correction * tail)], axis=0))
        keep = jnp.broadcast_to(jnp.exp(cum_end), (2 * HEAD, 2 * HEAD)).T
        values = v_ref[rows, wide]
        for head in range(2):
            lanes = slice(head * HEAD, (head + 1) * HEAD)
            query = side(*[q[:, lanes] for q in queries])
            near, rest = [s[:, lanes] for s in sources]
            scores = dot(side(query, query), side(near, near, rest, rest), NT)
            work.append(
                dict(
                    head=pair * 2 + head,
                    chunk=chunk,
                    query=query,
                    tail=tuple(t[:, lanes] for t in tails),
                    keep=keep[lanes, :],
                    value=jnp.concatenate(
                        [values[:, lanes], jnp.zeros((CHUNK, HEAD), jnp.bfloat16)], axis=1
                    ),
                    key_both=split(
                        jnp.concatenate(
                            [
                                jnp.where(strict, scores[:CHUNK, :CHUNK], 0.0),
                                jnp.where(causal, scores[CHUNK:, :CHUNK], 0.0),
                            ],
                            axis=0,
                        )
                    ),
                    pull=jnp.where(strict, scores[:CHUNK, CHUNK:], 0.0),
                    corr_read=split(jnp.where(causal, scores[CHUNK:, CHUNK:], 0.0)),
                )
            )
    for item in work:
        item["inverse"] = eye - jnp.where(row // 2 == col // 2, item["pull"], 0.0)
        item["from_values"] = dot(side(*item["key_both"]), stack(item["value"], item["value"]), NN)
    size = 2
    while size < CHUNK:
        joined = (row // (2 * size) == col // (2 * size)) & (row // size != col // size)
        halves = []
        for item in work:
            inverse = split(item["inverse"])
            between = split(jnp.where(joined, item["pull"], 0.0))
            halves.append((inverse, packed(side(*between), inverse)))
        for item, (inverse, half) in zip(work, halves):
            item["inverse"] = item["inverse"] - packed(side(*inverse), split(half))
        size *= 2
    key_row = lax.broadcasted_iota(jnp.int32, (HEAD, 2 * HEAD), 0)
    lane = lax.broadcasted_iota(jnp.int32, (HEAD, 2 * HEAD), 1)
    start = jnp.where(lane == key_row + HEAD, 1.0, 0.0)
    states = [start] * (2 * pairs)
    for item in work:
        head = item["head"]
        state = states[head]
        from_start = packed(item["query"], split(state)) + item["from_values"]
        pulled = packed(side(*split(item["inverse"])), split(from_start[:CHUNK]))
        pulled_parts = split(pulled)
        out_ref[pl.ds(item["chunk"] * CHUNK, CHUNK), pl.ds(head * 2 * HEAD, 2 * HEAD)] = (
            from_start[CHUNK:] - packed(side(*item["corr_read"]), pulled_parts)
        )
        key_tail = tuple(t[:CHUNK] for t in item["tail"])
        corr_tail = tuple(t[CHUNK:] for t in item["tail"])
        states[head] = (
            item["keep"] * state
            + dot2(key_tail, item["value"], TN)
            + dot3(corr_tail, pulled_parts, TN)
        )
    for head in range(2 * pairs):
        state_ref[pl.ds(head * HEAD, HEAD), :] = states[head].astype(jnp.bfloat16)


def route(place, ids_ref, weight_ref, pick_ref, high_ref, low_ref):
    tokens = ids_ref.shape[1]
    slots = N_SP * CAP
    expert = lax.broadcasted_iota(jnp.int32, (128, tokens), 0)
    named = [ids_ref[k : k + 1, :] == expert for k in range(2)]
    onehot = jnp.where(named[0] | named[1], 1.0, 0.0).astype(jnp.bfloat16)
    row = lax.broadcasted_iota(jnp.int32, (tokens, tokens), 0)
    col = lax.broadcasted_iota(jnp.int32, (tokens, tokens), 1)
    before = jnp.where(row < col, 1.0, 0.0).astype(jnp.bfloat16)
    earlier = dot(onehot, before, NN).astype(jnp.bfloat16)
    weight = jnp.where(named[0], weight_ref[0:1, :], 0.0) + jnp.where(named[1], weight_ref[1:2, :], 0.0)
    high, low = split(weight)
    slot = lax.broadcasted_iota(jnp.int32, (slots, 128), 0)
    source = lax.broadcasted_iota(jnp.int32, (slots, 128), 1)
    near = slot // (2 * CAP)
    step = NZ // 2 - (near + 1) // 2
    off = jnp.where(near % 2 == 1, step, NZ - step)
    chip = (place.z + off) % NZ
    core = (place.core + slot // CAP) % 2
    spread = jnp.where(source == chip * 2 + core, 1.0, 0.0).astype(jnp.bfloat16)
    rank = (lax.broadcasted_iota(jnp.int32, (slots, tokens), 0) % CAP).astype(jnp.float32)
    taken = jnp.where(dot(spread, earlier, NN) == rank, dot(spread, onehot, NN), 0.0)
    pick_ref[...] = taken.astype(jnp.bfloat16)
    high_ref[...] = (taken * dot(spread, high, NN)).astype(jnp.bfloat16)
    low_ref[...] = (taken * dot(spread, low, NN)).astype(jnp.bfloat16)


class Place:
    def __init__(self):
        self.sp = lax.axis_index("sp")
        self.tp = lax.axis_index("tp")
        self.z, self.core = self.sp // 2, self.sp % 2
        self.y, self.x = self.tp // SIDE, self.tp % SIDE

    def chip(self, off, other=False):
        core = (self.core + 1) % 2 if other else self.core
        return ((self.z + off + NZ) % NZ) * 2 + core

    def at_z(self, off, other=False):
        return {"sp": self.chip(off, other), "tp": self.tp}

    def along(self, axis, off):
        if axis == "x":
            return {"sp": self.sp, "tp": self.y * SIDE + (self.x + off + SIDE) % SIDE}
        return {"sp": self.sp, "tp": ((self.y + off + SIDE) % SIDE) * SIDE + self.x}

    def on(self, axis, off=0):
        return ((self.x if axis == "x" else self.y) + off + SIDE) % SIDE


class Copies:
    def __init__(self, send, recv):
        self.send, self.recv = send, recv
        self.made = []

    def __call__(self, src, dst, device):
        index = len(self.made)
        copy = pltpu.make_async_remote_copy(
            src_ref=src,
            dst_ref=dst,
            send_sem=self.send.at[index],
            recv_sem=self.recv.at[index],
            device_id=device,
            device_id_type=MESH,
        )
        self.made.append(copy)
        return copy

    def drain(self):
        for copy in self.made:
            copy.wait_send()


ORDER = (("x", "y"), ("y", "x"))


class TorusGather:
    def __init__(self, place, copies, blocks):
        self.place, self.copies, self.blocks = place, copies, blocks
        self.state = [dict() for _ in blocks]

    def at(self, h, first=0, second=0):
        one, two = ORDER[h]
        return self.place.on(two, second) * SIDE + self.place.on(one, first)

    def block(self, h, first=0, second=0):
        return self.blocks[h].at[self.at(h, first, second)]

    def row(self, h, second=0):
        start = self.place.on(ORDER[h][1], second) * SIDE
        return self.blocks[h].at[pl.ds(start, SIDE)]

    def begin(self, h):
        mine = self.block(h)
        sent = {off: self.copies(mine, mine, self.place.along(ORDER[h][0], off)) for off in (2, 1, -1)}
        for copy in sent.values():
            copy.start()
        self.state[h]["first"] = sent

    def arrive(self, h, off):
        self.state[h]["first"][off].wait_recv()

    def pair(self, h, ref):
        sent = [self.copies(ref, ref, self.place.along(ORDER[h][1], off)) for off in (1, -1)]
        for copy in sent:
            copy.start()
        return sent

    def relay(self, h, sent, ref_of, half):
        passed = []
        for side, (copy, off) in enumerate(zip(sent, (1, -1))):
            copy.wait_recv()
            piece = half(ref_of(-off), side)
            passed.append(self.copies(piece, piece, self.place.along(ORDER[h][1], off)))
            passed[-1].start()
        return passed


def front(
    place, copies, meanwhile,
    reads_ref, states_ref, gate_ref, gain_ref, weight_ref, residual_ref, out_ref,
    cores, maps, incoming_ref, halves,
):
    partner = place.at_z(0, True)
    tokens = out_ref.shape[0]
    heads = states_ref.shape[0] // HEAD
    mine = heads // 2
    cores[place.core] = states_ref[...]
    swap = copies(states_ref, cores.at[place.core], partner)
    swap.start()
    swap.wait_recv()
    for head in range(mine):
        rows = pl.ds(pl.multiple_of((place.core * mine + head) * HEAD, HEAD), HEAD)
        later = cores[1, rows, :]
        added = dot(later[:, HEAD:], cores[0, rows, :], NN)
        state = later[:, :HEAD].astype(jnp.float32) + added[:, :HEAD]
        maps[place.z, pl.ds(head * HEAD, HEAD), :] = jnp.concatenate(
            [state, added[:, HEAD:]], axis=1
        ).astype(jnp.bfloat16)

    came = {}
    last = {1: NZ // 2, -1: NZ // 2 - 1}

    def pass_on(direction, d):
        ref = maps.at[(place.z - direction * d + NZ) % NZ]
        for far in (2, 1):
            if d + far <= last[direction]:
                came[direction, d + far] = copies(ref, ref, place.at_z(direction * far))
                came[direction, d + far].start()

    def step_of(d, head):
        both = maps[(place.z - d + NZ) % NZ, pl.ds(head * HEAD, HEAD), :]
        return jnp.where(place.z >= d, both, unit)

    lane = lax.broadcasted_iota(jnp.int32, (HEAD, 2 * HEAD), 1)
    row = lax.broadcasted_iota(jnp.int32, (HEAD, 2 * HEAD), 0)
    identity = jnp.where(lane == row + HEAD, 1.0, 0.0)
    unit = identity.astype(jnp.bfloat16)
    window = [identity] * mine
    far = [jnp.zeros((HEAD, HEAD), jnp.float32)] * mine

    def take(direction, d):
        for head in range(mine):
            if direction > 0:
                both = step_of(d, head)
                hi, lo = split(window[head][:, HEAD:])
                added = dot(hi, both, NN) + dot(lo, both, NN)
                window[head] = side(window[head][:, :HEAD] + added[:, :HEAD], added[:, HEAD:])
            else:
                both = step_of(NZ - d, head)
                hi, lo = split(far[head])
                step_map = both[:, HEAD:]
                far[head] = (
                    both[:, :HEAD].astype(jnp.float32) + dot(step_map, hi, NN) + dot(step_map, lo, NN)
                )

    for d in range(0, NZ // 2, 2):
        for direction in (1, -1):
            if d:
                came[direction, d].wait_recv()
            pass_on(direction, d)
        if d:
            for direction in (1, -1):
                came[direction, d - 1].wait_recv()
                take(direction, d - 1)
                take(direction, d)
        if d // 2 < len(meanwhile):
            meanwhile[d // 2]()
    for direction in (1, -1):
        for d in (NZ // 2 - 1, NZ // 2):
            if d <= last[direction]:
                came[direction, d].wait_recv()
                take(direction, d)
    incoming = [
        window[head][:, :HEAD] + dot3(split(window[head][:, HEAD:]), split(far[head]))
        for head in range(mine)
    ]
    incoming_ref[place.core] = side(*incoming)
    swap = copies(incoming_ref.at[place.core], incoming_ref.at[place.core], partner)
    swap.start()
    second = (jnp.zeros((HEAD, HEAD), jnp.int32) + place.core) == 1
    swap.wait_recv()
    scaled = []
    for head in range(heads):
        before = incoming_ref[head // mine, :, (head % mine) * HEAD : (head % mine + 1) * HEAD]
        both = cores[0, pl.ds(head * HEAD, HEAD), :]
        hi, lo = split(before)
        step_map = both[:, HEAD:]
        after = both[:, :HEAD].astype(jnp.float32) + dot(step_map, hi, NN) + dot(step_map, lo, NN)
        state = jnp.where(second, after, before)
        both = reads_ref[:, pl.ds(head * 2 * HEAD, 2 * HEAD)]
        state_read = both[:, :HEAD] + dot3(split(both[:, HEAD:]), split(state))
        centred = state_read - jnp.mean(state_read, axis=1, keepdims=True)
        variance = jnp.mean(centred * centred, axis=1, keepdims=True)
        scaled.append(centred * lax.rsqrt(variance + EPS_GROUP))
    gated = (
        jnp.concatenate(scaled, axis=1)
        * gain_ref[...]
        * sigmoid(gate_ref[...].astype(jnp.float32))
    ).astype(jnp.bfloat16)
    gather = TorusGather(place, copies, halves)
    quarter = tokens // 4
    for h in range(2):
        for q in range(2):
            at = (2 * h + q) * quarter
            halves[h][gather.at(h), q] = gated[at : at + quarter]
    width = gated.shape[1]
    totals = [jnp.zeros((tokens // 2, out_ref.shape[1]), jnp.float32) for _ in range(2)]

    def project(h, first, second):
        x, y = (first, second) if h == 0 else (second, first)
        t = place.on("y", y) * SIDE + place.on("x", x)
        rows = pl.ds(pl.multiple_of(t * width, width), width)
        block = halves[h][gather.at(h, first, second)].reshape(tokens // 2, width)
        totals[h] += dot(block, weight_ref[rows, :], NN)

    pairs, passed = {}, {}
    for h in range(2):
        gather.begin(h)
    for h in range(2):
        pairs[h, 0] = gather.pair(h, gather.block(h))
    for off in (1, -1, 2):
        for h in range(2):
            gather.arrive(h, off)
            pairs[h, -off] = gather.pair(h, gather.block(h, -off))
    for first in (0, -1, 1, -2):
        for h in range(2):
            passed[h, first] = gather.relay(
                h, pairs[h, first],
                lambda second, h=h, first=first: gather.block(h, first, second),
                lambda ref, side: ref.at[side],
            )
        for h in range(2):
            project(h, first, 0)
            project(h, first, 1)
            project(h, first, -1)
    for first in (0, -1, 1, -2):
        for h in range(2):
            for copy in passed[h, first]:
                copy.wait_recv()
            project(h, first, 2)
    for h in range(2):
        part = pl.ds(h * (tokens // 2), tokens // 2)
        out_ref[part, :] = (residual_ref[part, :].astype(jnp.float32) + totals[h]).astype(jnp.bfloat16)


EXTRA = 128
SPREAD = ("y", "x")
SUM = ("x", "y")


def back_scratch(ff, features):
    quarter = ff // SIDE
    scratch = [pltpu.VMEM((N_SP, CAP, features), jnp.bfloat16) for _ in range(3)]
    for _ in range(2):
        scratch += [
            pltpu.VMEM((SIDE, features, 2 * quarter), jnp.bfloat16),
            pltpu.VMEM((PARTS, SIDE, 2, POS // 4 * CAP, features), jnp.bfloat16),
            pltpu.VMEM((PARTS, SIDE, SUB, 2 * quarter + EXTRA), jnp.bfloat16),
            pltpu.VMEM((PARTS, 3, SUB, 2 * quarter + EXTRA), jnp.bfloat16),
            pltpu.VMEM((PARTS, N_TP, 2, SUB // 2, quarter), jnp.bfloat16),
        ]
    return scratch


def spread_weights(place, copies, gain_ref, gate, up, scratch):
    gain = jnp.broadcast_to(gain_ref[...], (128, gain_ref.shape[1])).T[:, :1]
    quarter = gate.shape[1] // SIDE
    for matrix in (gate, up):
        matrix[...] = (matrix[...].astype(jnp.float32) * gain).astype(jnp.bfloat16)
    sent = []
    for h in range(2):
        target = scratch[3 + 5 * h]
        here = place.on(SPREAD[h])
        for n, matrix in enumerate((gate, up)):
            into = pl.ds(n * quarter, quarter)
            target[here, :, into] = matrix[:, pl.ds(pl.multiple_of(here * quarter, quarter), quarter)]
            for off in (2, 1, -1):
                columns = pl.ds(pl.multiple_of(place.on(SPREAD[h], off) * quarter, quarter), quarter)
                copy = copies(
                    matrix.at[:, columns], target.at[here, :, into], place.along(SPREAD[h], off)
                )
                copy.start()
                sent.append(copy)
    return sent


def peers_along_z(place):
    return [
        (2 * near + other, 2 * INVERSE[near] + other, place.at_z(off, bool(other)))
        for near, off in enumerate(OFFSETS)
        for other in range(2)
        if off != 0 or other
    ]


def back(
    place, copies, mid_ref, pick_ref, high_ref, low_ref, down_ref, out_ref, scratch,
):
    outgoing, results, returned = scratch[:3]
    weights, rows_in, products_of, others_of, hidden = zip(scratch[3:8], scratch[8:13])
    features = mid_ref.shape[1]
    quarter = hidden[0].shape[-1]
    z_peers = peers_along_z(place)

    def landing(at):
        part, i = at // POS, at % POS
        h, i = i // (POS // 2), i % (POS // 2)
        blocks = POS // 4
        return rows_in[h].at[part, place.on(SPREAD[h]), i // blocks, pl.ds(i % blocks * CAP, CAP)]

    dispatch = {}
    for part in range(PARTS):
        rows = pl.ds(part * POS * CAP, POS * CAP)
        outgoing[pl.ds(part * POS, POS)] = (
            dot(pick_ref[rows, :], mid_ref[...], NN).astype(jnp.bfloat16).reshape(POS, CAP, features)
        )
        for at, there, device in z_peers:
            if part * POS <= at < (part + 1) * POS:
                dispatch[at] = copies(outgoing.at[at], landing(there), device)
                dispatch[at].start()
    landing(HOME)[...] = outgoing[HOME]
    lands = {there: dispatch[at] for at, there, _ in z_peers}
    back = {}
    state = [dict() for _ in range(PARTS)]
    gathers = [
        TorusGather(place, copies, [hidden[h].at[part] for h in range(2)]) for part in range(PARTS)
    ]

    def gather_rows(part):
        for h in range(2):
            first = part * POS + h * (POS // 2)
            for at in range(first, first + POS // 2):
                if at in lands:
                    lands[at].wait_recv()
            mine = rows_in[h].at[part, place.on(SPREAD[h])]
            sent = [copies(mine, mine, place.along(SPREAD[h], off)) for off in (1, -1)]
            for copy in sent:
                copy.start()
            state[part][h, "rows"] = sent

    def relay_rows(part, h):
        sent = []
        for side, off in ((0, 1), (1, -1)):
            state[part][h, "rows"][side].wait_recv()
            piece = rows_in[h].at[part, place.on(SPREAD[h], -off), side]
            sent.append(copies(piece, piece, place.along(SPREAD[h], off)))
            sent[-1].start()
        state[part][h, "relayed"] = sent

    def multiply(part, h):
        for copy in state[part][h, "relayed"]:
            copy.wait_recv()
        total, squares = 0.0, 0.0
        for p in range(SIDE):
            rows = rows_in[h][part, p].reshape(POS // 2 * CAP, features)
            total += dot(rows, weights[h][p], NN)
            squares += jnp.sum(jnp.square(rows.astype(jnp.float32)), axis=1, keepdims=True)
        extra = jnp.broadcast_to(squares, (POS // 2 * CAP, EXTRA))
        value = jnp.concatenate([total, extra], axis=1).astype(jnp.bfloat16)
        products_of[h][part] = value.reshape(SIDE, SUB, 2 * quarter + EXTRA)
        sent = []
        for n, off in enumerate((2, 1, -1)):
            sent.append(
                copies(
                    products_of[h].at[part, place.on(SUM[h], off)],
                    others_of[h].at[part, n],
                    place.along(SUM[h], off),
                )
            )
            sent[-1].start()
        state[part][h, "products"] = sent

    def activate(part, h):
        for copy in state[part][h, "products"]:
            copy.wait_recv()
        total = products_of[h][part, place.on(SUM[h])].astype(jnp.float32)
        for n in range(3):
            total += others_of[h][part, n].astype(jnp.float32)
        inv = lax.rsqrt(total[:, 2 * quarter : 2 * quarter + 1] * (1.0 / D) + EPS_NORM)
        gate = total[:, :quarter] * inv
        value = gate * sigmoid(gate) * (total[:, quarter : 2 * quarter] * inv)
        gather = gathers[part]
        hidden[h][part, gather.at(h)] = value.astype(jnp.bfloat16).reshape(2, SUB // 2, quarter)
        gather.begin(h)

    def second_axis(part, h):
        for off in (1, -1, 2):
            gathers[part].arrive(h, off)
        state[part][h, "pair"] = gathers[part].pair(h, gathers[part].row(h))

    def relay_hidden(part, h):
        gather = gathers[part]
        state[part][h, "passed"] = gather.relay(
            h, state[part][h, "pair"],
            lambda second: gather.row(h, second), lambda ref, side: ref.at[:, side],
        )

    def outputs(part):
        for h in range(2):
            for copy in state[part][h, "passed"]:
                copy.wait_recv()
            total = 0.0
            for p in range(SIDE):
                rows = hidden[h][part, pl.ds(p * SIDE, SIDE)].reshape(POS // 2 * CAP, quarter)
                total += dot(rows, down_ref[pl.ds(p * quarter, quarter), :], NN)
            first = part * POS + h * (POS // 2)
            results[pl.ds(first, POS // 2)] = total.astype(jnp.bfloat16).reshape(POS // 2, CAP, features)
            for at, there, device in z_peers:
                if first <= at < first + POS // 2:
                    back[at] = copies(results.at[at], returned.at[there], device)
                    back[at].start()
        if part == HOME // POS:
            returned[HOME] = results[HOME]

    def both(action):
        def run(part):
            for h in range(2):
                action(part, h)
        return run

    stages = [
        gather_rows,
        both(relay_rows),
        both(multiply),
        both(activate),
        both(second_axis),
        both(relay_hidden),
        outputs,
    ]
    begins = (0.0, 7.0, 11.0, 13.0)
    plan = sorted(
        (begins[part] + 3.0 * n, part, n) for part in range(PARTS) for n in range(len(stages))
    )
    for _, part, n in plan:
        stages[n](part)

    came = {there: back[at] for at, there, _ in z_peers}
    total = mid_ref[...].astype(jnp.float32)
    for part in range(PARTS):
        for at in range(part * POS, (part + 1) * POS):
            if at in came:
                came[at].wait_recv()
        rows = returned[pl.ds(part * POS, POS)].reshape(POS * CAP, features)
        columns = pl.ds(part * POS * CAP, POS * CAP)
        total += dot(high_ref[columns, :], rows, TN) + dot(low_ref[columns, :], rows, TN)
    out_ref[...] = total


def kernel(
    r_ref, k_ref, v_ref, d_ref, a_ref, gate_logits_ref, group_gain_ref, residual_ref, norm_gain_ref,
    ids_ref, route_weight_ref, mixer_hbm, gate_hbm, up_hbm, down_hbm, out_ref, *scratch
):
    mixer, gate, up, down, loaded, send, recv = scratch[:7]
    reads, states, pick, high, low, midway, cores, maps, incoming = scratch[7:16]
    halves = scratch[16:18]
    place = Place()
    copies = Copies(send, recv)
    barrier = pltpu.get_barrier_semaphore()
    others = [peer[2] for peer in peers_along_z(place)]
    others += [place.along(axis, off) for axis in "xy" for off in (2, 1, -1)]
    for device in others:
        pl.semaphore_signal(barrier, inc=1, device_id=device, device_id_type=MESH)
    loads = [
        pltpu.make_async_copy(src, dst, loaded.at[n])
        for n, (src, dst) in enumerate(
            [(mixer_hbm, mixer), (gate_hbm, gate), (up_hbm, up), (down_hbm, down)]
        )
    ]
    for load in loads:
        load.start()
    mix(r_ref, k_ref, v_ref, d_ref, a_ref, reads, states)
    pl.semaphore_wait(barrier, len(others))

    spread = []

    def prepare_weights():
        for load in loads:
            load.wait()
        spread.extend(spread_weights(place, copies, norm_gain_ref, gate, up, scratch[18:]))

    meanwhile = [
        lambda: route(place, ids_ref, route_weight_ref, pick, high, low),
        prepare_weights,
    ]
    front(
        place, copies, meanwhile,
        reads, states, gate_logits_ref, group_gain_ref, mixer, residual_ref, midway,
        cores, maps, incoming, halves,
    )
    for copy in spread:
        copy.wait_recv()
    back(place, copies, midway, pick, high, low, down, out_ref, scratch[18:])
    copies.drain()


def local(
    receptance,
    key_vectors,
    value_vectors,
    decay_logits,
    rate_logits,
    gate_logits,
    group_gain,
    residual,
    mixer_out,
    norm_gain,
    expert_ids,
    route_weight,
    expert_gate,
    expert_up,
    expert_down,
):
    tokens, channels = residual.shape
    features = norm_gain.shape[0]
    ff = expert_gate.shape[2]
    slots = N_SP * CAP
    count = 2 + (NZ - 1) + 12 + 38 + 2 * (N_SP - 1) + PARTS * 28
    bf16 = jnp.bfloat16
    vmem = pl.BlockSpec(memory_space=pltpu.VMEM)
    hbm = pl.BlockSpec(memory_space=pl.ANY)
    weights = (mixer_out, expert_gate[0], expert_up[0], expert_down[0])
    return pl.pallas_call(
        kernel,
        in_specs=[vmem] * 11 + [hbm] * 4,
        out_specs=vmem,
        out_shape=jax.ShapeDtypeStruct((tokens, features), jnp.float32),
        scratch_shapes=[pltpu.VMEM(w.shape, bf16) for w in weights]
        + [
            pltpu.SemaphoreType.DMA((len(weights),)),
            pltpu.SemaphoreType.DMA((count,)),
            pltpu.SemaphoreType.DMA((count,)),
            pltpu.VMEM((tokens, 2 * channels), jnp.float32),
            pltpu.VMEM((channels, 2 * HEAD), bf16),
            pltpu.VMEM((slots, tokens), bf16),
            pltpu.VMEM((slots, tokens), bf16),
            pltpu.VMEM((slots, tokens), bf16),
            pltpu.VMEM((tokens, features), bf16),
            pltpu.VMEM((2, channels, 2 * HEAD), bf16),
            pltpu.VMEM((NZ, channels // 2, 2 * HEAD), bf16),
            pltpu.VMEM((2, HEAD, channels // 2), jnp.float32),
            pltpu.VMEM((N_TP, 2, tokens // 4, channels), bf16),
            pltpu.VMEM((N_TP, 2, tokens // 4, channels), bf16),
        ]
        + back_scratch(ff, features),
        compiler_params=pltpu.CompilerParams(
            collective_id=0, has_side_effects=True, vmem_limit_bytes=60 * 1024 * 1024
        ),
        name="layer",
    )(
        receptance, key_vectors, value_vectors, decay_logits, rate_logits, gate_logits,
        group_gain.reshape(1, channels), residual, norm_gain.reshape(1, features),
        expert_ids.T, route_weight.T, *weights,
    ).astype(bf16)


def solution(mesh):
    placed = (
        P("sp", "tp"),
        P("sp", "tp"),
        P("sp", "tp"),
        P("sp", "tp"),
        P("sp", "tp"),
        P("sp", "tp"),
        P("tp"),
        P("sp", "tp"),
        P(None, "tp"),
        P("tp"),
        P("sp", None),
        P("sp", None),
        P("sp", "tp", None),
        P("sp", "tp", None),
        P("sp", None, "tp"),
    )
    return jax.shard_map(
        local, mesh=mesh, in_specs=placed, out_specs=P("sp", "tp"), check_vma=False
    )
```
